32 devices in a mesh: kv: 8 (over z, y), tp: 4 (over x, core).
Axes of the slice: x: 2, y: 2, z: 4, core: 2. Of those that a mesh axis runs over, the one named last changes fastest.
Arguments:
- hidden: bfloat16 [128, 4096], P(None, 'tp'), may hold values from -50 to 50
- input_gain: bfloat16 [4096], P('tp'), may hold values from 0.099609375 to 1.8984375
- x_weight: bfloat16 [4096, 8192], P('tp', 'kv'), may hold values from -0.09375 to 0.09375
- z_weight: bfloat16 [4096, 8192], P('tp', 'kv'), may hold values from -0.09375 to 0.09375
- bc_weight: bfloat16 [4096, 8192], P('tp', 'kv'), may hold values from -0.09375 to 0.09375
- dt_weight: bfloat16 [4096, 128], P('tp', 'kv'), may hold values from -0.09375 to 0.09375
- x_kernel: bfloat16 [4, 8192], P(None, 'kv'), may hold values from -3 to 3
- bc_kernel: bfloat16 [4, 8192], P(None, 'kv'), may hold values from -3 to 3
- dt_bias: float32 [128], P('kv'), may hold values from -3 to 0.5
- decay_log: float32 [128], P('kv'), may hold values from -3 to 1.5
- skip_scale: float32 [128], P('kv'), may hold values from 0.5 to 1.5
- output_gain: bfloat16 [8192], P('kv'), may hold values from 0.099609375 to 1.8984375
- output_weight: bfloat16 [8192, 4096], P('kv'), may hold values from -0.09375 to 0.09375
- saved_states: float32 [32, 5, 128, 64, 128], P('tp', None, 'kv'), may hold values from -1.8 to 1.8
- x_history: bfloat16 [32, 7, 8192], P('tp', None, 'kv'), may hold values from -6 to 6
- bc_history: bfloat16 [32, 7, 8192], P('tp', None, 'kv'), may hold values from -6 to 6
- accepted: int32 [32], P('tp'), may hold values from 0 to 4
Outputs:
- mixed: bfloat16 [128, 4096], P('tp', 'kv')
- new_states: float32 [32, 5, 128, 64, 128], P('tp', None, 'kv')
- x_window: bfloat16 [32, 7, 8192], P('tp', None, 'kv')
- bc_window: bfloat16 [32, 7, 8192], P('tp', None, 'kv')
The draws below stay inside these ranges and needn't reach their ends.
All inputs are finite; a program needn't handle non-finite values.
Results may differ from the reference program's by a relative error of at most 0.02.
Values may be sent and summed in bfloat16 or wider, within the bound.
A program may use at most 192 MiB of HBM per device.

```python
import jax
import jax.numpy as jnp
from jax import lax

D = 4096
HEADS = 128
HEAD_SIZE = 64
STATE = 128
GROUPS = 32
CONV = 4
PROPS = 4
SEQS = 32
TOKENS = 128
INNER = 8192
BC_WIDTH = 8192
HIST = 7
FEATURE_BLOCKS = 4


def draw_hidden(key, part):
    noise_key = jax.random.fold_in(key, 0)
    samples = jnp.clip(jax.random.normal(noise_key, (TOKENS, D), jnp.float32), -6.0, 6.0)
    quarter = jnp.arange(D) * 4 // D
    factors = jnp.array([0.5, 1.6, 0.4, 1.2], jnp.float32)[quarter]
    return (samples * factors[None, :]).astype(jnp.bfloat16)


def set_ends(result, rng, smallest, top_value):
    longest = result.shape.index(max(result.shape))
    spots = []
    for shift in (0, 1):
        where = [jax.random.randint(jax.random.fold_in(rng, axis), (), 0, length) for axis, length in enumerate(result.shape)]
        where[longest] = (where[longest] + shift) % result.shape[longest]
        spots.append(tuple(where))
    return result.at[spots[0]].set(smallest).at[spots[1]].set(top_value)


def with_spikes(entries, rng, source, target, shards_of, factor):
    owner, partner = [(jnp.arange(entries.shape[dim]) // (entries.shape[dim] // shards_of)).reshape([-1 if axis == dim else 1 for axis in range(entries.ndim)]) for dim in (source, target)]
    chosen = jax.random.permutation(rng, shards_of)[partner]
    strong = (owner == chosen) | (owner == (partner + shards_of // 2) % shards_of)
    return jnp.where(strong, factor * entries, entries)


def level_of(rng, extent, shards, low, top_value):
    gain = 1.0
    for axis_at, blocks in shards:
        draws = jax.random.uniform(jax.random.fold_in(jax.random.fold_in(rng, 6), axis_at), (blocks,), jnp.float32, low / len(shards), top_value / len(shards))
        gain = gain * jnp.repeat(jnp.exp(draws), extent[axis_at] // blocks).reshape((-1,) + (1,) * (len(extent) - 1 - axis_at))
    return gain


def bell_draw(key, dims, width, limit, cuts=(), kind=jnp.bfloat16):
    gain = level_of(key, dims, cuts, -0.22, 0.18) if cuts else 1.0
    values = jax.random.normal(key, dims, jnp.float32) * width * gain
    return jnp.minimum(jnp.maximum(values, -limit), limit).astype(kind)


def noise_with(stream_key, extent, spread, reach, cuts, heavy, kind=jnp.bfloat16):
    result = spread * jax.random.normal(stream_key, extent, jnp.float32)
    if cuts:
        result = result * level_of(stream_key, extent, cuts, -0.22, 0.18)
    return jnp.clip(with_spikes(result, jax.random.fold_in(stream_key, 3), *heavy), -reach, reach).astype(kind)


def setup_inputs(seed: int = 0) -> dict:
    streams_of = jax.random.split(jax.random.key(seed), 18)
    return {
        "hidden": draw_hidden(jax.random.fold_in(streams_of[17], 71), 0),
        "input_gain": jnp.clip(1.0 + 0.18 * jax.random.normal(streams_of[1], (D,), jnp.float32), 0.099609375, 1.8984375).astype(jnp.bfloat16),
        "x_weight": bell_draw(streams_of[2], (D, INNER), D ** -0.5, 0.09375, ((0, 4), (1, 8))),
        "z_weight": bell_draw(streams_of[3], (D, INNER), D ** -0.5, 0.09375, ((0, 4), (1, 8))),
        "bc_weight": bell_draw(streams_of[4], (D, BC_WIDTH), D ** -0.5, 0.09375, ((0, 4), (1, 8))),
        "dt_weight": bell_draw(streams_of[5], (D, HEADS), D ** -0.5, 0.09375, ((0, 4), (1, 8))),
        "x_kernel": bell_draw(streams_of[6], (CONV, INNER), CONV ** -0.5, 3.0, ((1, 8),)),
        "bc_kernel": bell_draw(streams_of[7], (CONV, BC_WIDTH), CONV ** -0.5, 3.0, ((1, 8),)),
        "dt_bias": jnp.clip(-3.0 + 3.5 * jax.random.uniform(streams_of[8], (HEADS,), jnp.float32) ** level_of(streams_of[8], (HEADS,), ((0, 8),), -0.2, 0.2), -3.0, 0.5),
        "decay_log": jnp.clip(-3.0 + 4.5 * jax.random.uniform(streams_of[9], (HEADS,), jnp.float32) ** level_of(streams_of[9], (HEADS,), ((0, 8),), -0.2, 0.2), -3.0, 1.5),
        "skip_scale": jnp.clip(0.5 + 1.0 * jax.random.uniform(streams_of[10], (HEADS,), jnp.float32) ** level_of(streams_of[10], (HEADS,), ((0, 8),), -0.2, 0.2), 0.5, 1.5),
        "output_gain": jnp.clip(1.0 + 0.18 * jax.random.normal(streams_of[11], (INNER,), jnp.float32), 0.099609375, 1.8984375).astype(jnp.bfloat16),
        "output_weight": noise_with(streams_of[12], (INNER, D), INNER ** -0.5, 0.09375, ((0, 8),), (0, 1, 8, 2.0)),
        "saved_states": bell_draw(streams_of[13], (SEQS, PROPS + 1, HEADS, HEAD_SIZE, STATE), 0.3, 1.8, ((0, 4), (2, 8)), jnp.float32),
        "x_history": bell_draw(streams_of[14], (SEQS, HIST, INNER), 1.0, 6.0, ((0, 4), (2, 8))),
        "bc_history": bell_draw(streams_of[15], (SEQS, HIST, BC_WIDTH), 1.0, 6.0, ((0, 4), (2, 8))),
        "accepted": set_ends(jax.random.randint(streams_of[16], (SEQS,), 0, PROPS + 1), jax.random.fold_in(streams_of[16], 1), 0, PROPS).astype(jnp.int32),
    }


EPSILON = 1e-05

def take_window(history, accepted, fresh_rows):
    history_len = history.shape[1] - fresh_rows.shape[1]
    indices = accepted[:, None] + jnp.arange(history_len, dtype=jnp.int32)[None, :]
    kept_rows = jnp.take_along_axis(history, indices[:, :, None], axis=1)
    return jnp.concatenate([kept_rows, fresh_rows], axis=1)

def conv_silu(window, kernel):
    length = window.shape[1] - kernel.shape[0] + 1
    running = window[:, 0:length].astype(jnp.float32) * kernel[0].astype(jnp.float32)
    for offset in range(1, kernel.shape[0]):
        running = running + window[:, offset:offset + length].astype(jnp.float32) * kernel[offset].astype(jnp.float32)
    return jax.nn.silu(running)

def ssd_block(x_conv, step_size, decay_rate, b_terms, c_terms, first_state, skip_scale):
    cumulated = jnp.cumsum(-decay_rate * step_size, axis=1)
    length = x_conv.shape[1]
    indices = jnp.arange(length)
    causal = indices[:, None] >= indices[None, :]
    gaps = cumulated[:, :, None, :] - cumulated[:, None, :, :]
    weights = jnp.exp(jnp.where(causal[None, :, :, None], gaps, -jnp.inf))
    inputs = x_conv * step_size[..., None]
    outer_prod = jnp.einsum('srhp,srhn->srhpn', inputs, b_terms)
    states = jnp.exp(cumulated)[..., None, None] * first_state[:, None] + jnp.einsum('strh,srhpn->sthpn', weights, outer_prod)
    output = jnp.einsum('sthn,sthpn->sthp', c_terms, states) + skip_scale[:, None] * x_conv
    return (output, states)

def reference(hidden, input_gain, x_weight, z_weight, bc_weight, dt_weight, x_kernel, bc_kernel, dt_bias, decay_log, skip_scale, output_gain, output_weight, saved_states, x_history, bc_history, accepted):
    widened = hidden.astype(jnp.float32)
    normed = (widened * lax.rsqrt(lax.optimization_barrier(jnp.mean(widened * widened, axis=1, keepdims=True)) + EPSILON) * input_gain.astype(jnp.float32)).astype(jnp.bfloat16)
    weights = jnp.concatenate([x_weight, z_weight, bc_weight, dt_weight], axis=1)
    feature_block = D // FEATURE_BLOCKS
    running = jnp.zeros((normed.shape[0], weights.shape[1]), jnp.float32)
    for part_index in range(FEATURE_BLOCKS):
        product = jnp.dot(normed[:, part_index * feature_block:(part_index + 1) * feature_block], weights[part_index * feature_block:(part_index + 1) * feature_block], preferred_element_type=jnp.float32)
        running = running + lax.optimization_barrier(product.astype(jnp.bfloat16)).astype(jnp.float32)
    projected = running.astype(jnp.bfloat16)
    x_fresh = projected[:, :INNER]
    z_fresh = projected[:, INNER:2 * INNER]
    bc_fresh = projected[:, 2 * INNER:2 * INNER + BC_WIDTH]
    dt_fresh = projected[:, 2 * INNER + BC_WIDTH:]
    x_window = take_window(x_history, accepted, x_fresh.reshape(SEQS, PROPS, INNER))
    bc_window = take_window(bc_history, accepted, bc_fresh.reshape(SEQS, PROPS, BC_WIDTH))
    x_conv = conv_silu(x_window, x_kernel).reshape(SEQS, PROPS, HEADS, HEAD_SIZE)
    bc_conv = conv_silu(bc_window, bc_kernel).reshape(SEQS, PROPS, GROUPS, 2, STATE)
    b_terms = jnp.repeat(bc_conv[:, :, :, 0], HEADS // GROUPS, axis=2)
    c_terms = jnp.repeat(bc_conv[:, :, :, 1], HEADS // GROUPS, axis=2)
    step_size = jax.nn.softplus(dt_fresh.astype(jnp.float32).reshape(SEQS, PROPS, HEADS) + dt_bias)
    first_state = jnp.take_along_axis(saved_states, accepted[:, None, None, None, None], axis=1)[:, 0]
    decay_rate = jnp.exp(decay_log)

    def one_sequence(pieces):
        x_one, step_one, b_one, c_one, state_one = pieces
        out_one, states_one = ssd_block(x_one[None], step_one[None], decay_rate, b_one[None], c_one[None], state_one[None], skip_scale)
        return (out_one[0], states_one[0])
    output, states = lax.map(one_sequence, (x_conv, step_size, b_terms, c_terms, first_state))
    new_states = jnp.concatenate([first_state[:, None], states], axis=1)
    gate_values = z_fresh.astype(jnp.float32).reshape(SEQS, PROPS, HEADS, HEAD_SIZE)
    gated = (output * jax.nn.silu(gate_values)).reshape(TOKENS, INNER)
    scaled = (gated * output_gain.astype(jnp.float32)).astype(jnp.bfloat16)
    branch = jnp.dot(scaled, output_weight, preferred_element_type=jnp.float32)
    mixed = (lax.rsqrt(lax.optimization_barrier(jnp.mean(gated * gated, axis=1)) + EPSILON)[:, None] * branch).astype(jnp.bfloat16)
    return (mixed, new_states, x_window, bc_window)
```

```python
import jax
import jax.numpy as jnp
import functools

from jax import lax
from jax.experimental import pallas as pl
from jax.experimental.pallas import tpu as pltpu
from jax.sharding import PartitionSpec as P

D = 4096
PROPS = 4
INNER = 8192


EPSILON = 1e-05


def partner_2(block, axis, stride):
    count = lax.axis_size(axis)
    route = []
    for low in range(count):
        high = low | 1 << stride
        if high != low and high < count:
            route += [(low, high), (high, low)]
    return lax.ppermute(block, axis, route)


def take_window(history, accepted, fresh_rows):
    history_len = history.shape[1] - fresh_rows.shape[1]
    indices = accepted[:, None] + jnp.arange(history_len, dtype=jnp.int32)[None, :]
    kept_rows = jnp.take_along_axis(history, indices[:, :, None], axis=1)
    return jnp.concatenate([kept_rows, fresh_rows], axis=1)


def conv_silu(window, kernel):
    length = window.shape[1] - kernel.shape[0] + 1
    running = window[:, 0:length].astype(jnp.float32) * kernel[0].astype(jnp.float32)
    for offset in range(1, kernel.shape[0]):
        running = running + window[:, offset : offset + length].astype(jnp.float32) * kernel[
            offset
        ].astype(jnp.float32)
    return jax.nn.silu(running)


def ssd_block(x_conv, step_size, decay_rate, b_terms, c_terms, first_state, skip_scale):
    cumulated = jnp.cumsum(-decay_rate * step_size, axis=1)
    length = x_conv.shape[1]
    indices = jnp.arange(length)
    causal = indices[:, None] >= indices[None, :]
    gaps = cumulated[:, :, None, :] - cumulated[:, None, :, :]
    weights = jnp.exp(jnp.where(causal[None, :, :, None], gaps, -jnp.inf))
    inputs = x_conv * step_size[..., None]
    outer_prod = jnp.einsum("srhp,srhn->srhpn", inputs, b_terms)
    states = jnp.exp(cumulated)[..., None, None] * first_state[:, None] + jnp.einsum(
        "strh,srhpn->sthpn", weights, outer_prod
    )
    output = jnp.einsum("sthn,sthpn->sthp", c_terms, states) + skip_scale[:, None] * x_conv
    return (output, states)


def local_general(
    hidden,
    input_gain,
    x_weight,
    z_weight,
    bc_weight,
    dt_weight,
    x_kernel,
    bc_kernel,
    dt_bias,
    decay_log,
    skip_scale,
    output_gain,
    output_weight,
    saved_states,
    x_history,
    bc_history,
    accepted,
):
    heads_here = dt_bias.shape[0]
    head_size = x_weight.shape[1] // heads_here
    state_size = saved_states.shape[4]
    seqs_here = accepted.shape[0]
    rows_here = hidden.shape[0] // lax.axis_size("tp")
    inner_here = x_weight.shape[1]
    bc_here = bc_weight.shape[1]
    widened = hidden.astype(jnp.float32)
    squares = lax.psum(jnp.sum(widened * widened, axis=1), "tp")
    normed = (
        widened * lax.rsqrt(squares[:, None] / D + EPSILON) * input_gain.astype(jnp.float32)
    ).astype(jnp.bfloat16)
    weights = jnp.concatenate([x_weight, z_weight, bc_weight, dt_weight], axis=1)
    product = jnp.dot(normed, weights, preferred_element_type=jnp.float32)
    projected = lax.psum_scatter(
        lax.optimization_barrier(product.astype(jnp.bfloat16))
        .astype(jnp.float32)
        .astype(jnp.bfloat16),
        "tp",
        scatter_dimension=0,
        tiled=True,
    )
    x_fresh = projected[:, :inner_here]
    z_fresh = projected[:, inner_here : 2 * inner_here]
    bc_fresh = projected[:, 2 * inner_here : 2 * inner_here + bc_here]
    dt_fresh = projected[:, 2 * inner_here + bc_here :]
    x_window = take_window(x_history, accepted, x_fresh.reshape(seqs_here, PROPS, inner_here))
    bc_window = take_window(bc_history, accepted, bc_fresh.reshape(seqs_here, PROPS, bc_here))
    x_conv = conv_silu(x_window, x_kernel).reshape(seqs_here, PROPS, heads_here, head_size)
    bc_conv = conv_silu(bc_window, bc_kernel)
    spread = max(4 // heads_here, 1)
    position = lax.axis_index("kv")
    for level in range(spread.bit_length() - 1):
        partner = partner_2(bc_conv, "kv", level)
        low_half = position // 2**level % 2 == 0
        bc_conv = jnp.where(
            low_half,
            jnp.concatenate([bc_conv, partner], axis=2),
            jnp.concatenate([partner, bc_conv], axis=2),
        )
    groups_here = bc_conv.shape[2] // (2 * state_size)
    paired = bc_conv.reshape(seqs_here, PROPS, groups_here, 2, state_size)
    per_group = heads_here // groups_here
    b_terms = jnp.repeat(paired[:, :, :, 0], per_group, axis=2)
    c_terms = jnp.repeat(paired[:, :, :, 1], per_group, axis=2)
    step_size = jax.nn.softplus(
        dt_fresh.astype(jnp.float32).reshape(seqs_here, PROPS, heads_here) + dt_bias
    )
    first_state = jnp.take_along_axis(saved_states, accepted[:, None, None, None, None], axis=1)[
        :, 0
    ]
    output, states = ssd_block(
        x_conv, step_size, jnp.exp(decay_log), b_terms, c_terms, first_state, skip_scale
    )
    new_states = jnp.concatenate([first_state[:, None], states], axis=1)
    gate_values = z_fresh.astype(jnp.float32).reshape(seqs_here, PROPS, heads_here, head_size)
    gated = (output * jax.nn.silu(gate_values)).reshape(rows_here, inner_here)
    square_sum = jnp.sum(gated * gated, axis=1)
    scaled = (gated * output_gain.astype(jnp.float32)).astype(jnp.bfloat16)
    partial_value = jnp.dot(scaled, output_weight, preferred_element_type=jnp.float32)
    total_squares = lax.psum(square_sum, "kv")
    summed = lax.psum_scatter(partial_value, "kv", scatter_dimension=1, tiled=True)
    mixed = (lax.rsqrt(total_squares / INNER + EPSILON)[:, None] * summed).astype(jnp.bfloat16)
    return (mixed, new_states, x_window, bc_window)


NN = (((1,), (0,)), ((), ()))
NT = (((1,), (1,)), ((), ()))
CHUNK = 512
LAG = 3


def dot(a, b, dims=NN, **kw):
    return lax.dot_general(a, b, dims, preferred_element_type=jnp.float32, **kw)


def silu(v):
    return v / (1.0 + jnp.exp(-v))


def softplus(v):
    return jnp.maximum(v, 0.0) + jnp.log(1.0 + jnp.exp(-jnp.abs(v)))


def flip(index, mask):
    out = index
    bit = 1
    while bit <= mask:
        if mask & bit:
            out = out + bit - 2 * bit * lax.rem(index // bit, 2)
        bit *= 2
    return out


def remote(src, dst, send_sem, recv_sem, device):
    return pltpu.make_async_remote_copy(
        src_ref=src, dst_ref=dst, send_sem=send_sem, recv_sem=recv_sem,
        device_id=device, device_id_type=pl.DeviceIdType.MESH)


def main_kernel(
    features, channels, n_kv,
    acc_smem, bias_smem, decay_smem, skip_smem,
    hid_hbm, gin_ref, xw_hbm, zw_hbm, bcw_hbm, dtw_hbm, xh_ref, bch_ref, xk_ref, bck_ref, gain_ref,
    saved_hbm, w_hbm,
    mixed_ref, s0_ref, xdt_ref, b_ref, a_ref, xwin_ref, bcwin_ref,
    hid, entry32, dtw, wbuf, prod_dt, prod, peer_dt, peer, half_dt, half, own_dt, own, far_dt, far,
    w_buf, part, slots, norm_out, norm_in, fin,
    hid_sem, w_sem, saved_sem, ow_sem, c_send, c_recv, x_send, x_recv, o_send, o_recv, n_send, n_recv,
    *saved,
):
    seqs = acc_smem.shape[0]
    rows = mixed_ref.shape[0]
    props = rows // seqs
    tokens = hid.shape[0]
    inner = xwin_ref.shape[2]
    _, heads, size, state = saved[0].shape
    groups = bcwin_ref.shape[2] // (2 * state)
    per = heads // groups
    span = per * size
    n_chunk = inner // CHUNK
    in_chunk = CHUNK // span
    block = mixed_ref.shape[1]

    kv, tp = lax.axis_index("kv"), lax.axis_index("tp")
    side, core = tp // 2, lax.rem(tp, 2)
    core_peer, x_peer = flip(tp, 1), flip(tp, 2)
    exits = [flip(kv, d) for d in range(n_kv - 1, 0, -1)]

    barrier = pltpu.get_barrier_semaphore()
    for device in [{"tp": core_peer}, {"tp": x_peer}] + [{"kv": p} for p in exits]:
        pl.semaphore_signal(barrier, inc=1, device_id=device, device_id_type=pl.DeviceIdType.MESH)

    hid_copy = pltpu.make_async_copy(hid_hbm, hid, hid_sem.at[0])
    hid_copy.start()
    dtw_copy = pltpu.make_async_copy(dtw_hbm, dtw.at[pl.ds(0, heads)], hid_sem.at[1])
    dtw_copy.start()
    w_copies = [
        pltpu.make_async_copy(src.at[:, pl.ds(j * CHUNK, CHUNK)], wbuf.at[i], w_sem.at[i])
        for i, (src, j) in enumerate(
            [(src, j) for src in (bcw_hbm, xw_hbm, zw_hbm) for j in range(n_chunk)])
    ]
    for copy in w_copies:
        copy.start()
    n_big = len(w_copies)

    dtw[heads:] = jnp.zeros((dtw.shape[0] - heads, dtw.shape[1]), dtw.dtype)
    hid_copy.wait()
    lanes = entry32.shape[2]
    for i in range(entry32.shape[0]):
        entry32[i] = hid[:, i * lanes : (i + 1) * lanes].astype(jnp.float32)
    gin = gin_ref[...].astype(jnp.float32).reshape(1, -1)
    entry, squares = [], []
    for p in range(tokens // rows):
        for t in range(props):
            v = jnp.concatenate(
                [entry32[i, pl.ds(p * rows + t, seqs, stride=props), :] for i in range(entry32.shape[0])],
                axis=1)
            squares.append(jnp.sum(v * v, axis=1, keepdims=True))
            entry.append(v * gin)
    entry = jnp.concatenate(entry, axis=0).astype(jnp.bfloat16)
    squares = jnp.concatenate(squares, axis=0)
    high = squares.astype(jnp.bfloat16).astype(jnp.float32)

    saved_copies = [
        pltpu.make_async_copy(saved_hbm.at[s], saved[s], saved_sem.at[s]) for s in range(seqs)]
    ow_copies = [
        pltpu.make_async_copy(
            w_hbm.at[:, pl.ds(pl.multiple_of(p * block, block), block)], w_buf.at[i], ow_sem.at[i])
        for i, p in enumerate(exits + [kv])]

    def put(ref, value):
        for p in range(tokens // rows):
            ref[(p % 2) * 2 + p // 2] = value[p * rows : (p + 1) * rows].astype(jnp.bfloat16)

    def core_copy(k):
        src, dst = (prod_dt, peer_dt) if k < 0 else (prod.at[k], peer.at[k])
        return remote(
            src.at[pl.ds(2 - 2 * core, 2)], dst, c_send.at[k + 1], c_recv.at[k + 1], {"tp": core_peer})

    def x_copy(k):
        src, dst = (half_dt, far_dt) if k < 0 else (half.at[k], far.at[k])
        return remote(src, dst, x_send.at[k + 1], x_recv.at[k + 1], {"tp": x_peer})

    def forward(k):
        core_copy(k).wait_recv()
        mine, theirs, send, keep = (prod_dt, peer_dt, half_dt, own_dt) if k < 0 else (
            prod.at[k], peer.at[k], half.at[k], own.at[k])
        away = mine[2 * core + 1 - side].astype(jnp.float32) + theirs[1 - side].astype(jnp.float32)
        send[...] = away.astype(jnp.bfloat16)
        x_copy(k).start()
        keep[...] = mine[2 * core + side].astype(jnp.float32) + theirs[side].astype(jnp.float32)

    dtw_copy.wait()
    lane = lax.broadcasted_iota(jnp.int32, (tokens, 128), 1)
    first = dot(entry, dtw[...], NT)
    first = jnp.where(lane == 126, high, jnp.where(lane == 127, squares - high, first))
    put(prod_dt, first)
    pl.semaphore_wait(barrier, 2 + len(exits))
    core_copy(-1).start()
    for k in range(n_big):
        w_copies[k].wait()
        put(prod.at[k], dot(entry, wbuf[k]))
        core_copy(k).start()
        if k >= LAG - 1:
            forward(k - LAG)
        if k == n_big - 1:
            for copy in saved_copies + ow_copies:
                copy.start()
    for k in range(n_big - LAG, n_big):
        forward(k)

    seq_at = lax.broadcasted_iota(jnp.int32, (seqs, CHUNK), 0)
    acc = jnp.zeros((seqs, CHUNK), jnp.int32)
    for s in range(seqs):
        acc = jnp.where(seq_at == s, acc_smem[s], acc)
    picks = [acc == j for j in range(props + 1)]
    eh = lax.broadcasted_iota(jnp.int32, (128, inner), 0)
    ec = lax.broadcasted_iota(jnp.int32, (128, inner), 1)
    expand = (eh == ec // size).astype(jnp.float32)
    lane_at = lax.broadcasted_iota(jnp.int32, (8, 128), 1)
    row_at = lax.broadcasted_iota(jnp.int32, (8, 128), 0)
    par = jnp.zeros((8, 128), jnp.float32)
    for i, smem in enumerate((bias_smem, decay_smem, skip_smem)):
        for h in range(heads):
            par = jnp.where((row_at == i) & (lane_at == h), smem[h], par)
    wide = dot(par, expand, precision=lax.Precision.HIGHEST)
    bias, rate, skip = wide[0:1], jnp.exp(wide[1:2]), wide[2:3]
    row = lax.broadcasted_iota(jnp.int32, (rows, state), 0)

    def total(k):
        x_copy(k).wait_recv()
        if k < 0:
            return own_dt[...] + far_dt[...].astype(jnp.float32)
        return own[k] + far[k].astype(jnp.float32)

    head_part = total(-1)
    sums = head_part[:, 126:127] + head_part[:, 127:128]
    scale = lax.rsqrt(sums / features + EPSILON)

    def fresh(k):
        v = (total(k) * scale).astype(jnp.bfloat16).astype(jnp.float32)
        return [v[t * seqs : (t + 1) * seqs] for t in range(props)]

    def conv(hist_ref, tap_ref, out_ref, rows_fresh, lo):
        kept = hist_ref.shape[0] - props
        hist = [hist_ref[m, :, lo : lo + CHUNK].astype(jnp.float32) for m in range(hist_ref.shape[0])]
        win = []
        for k in range(kept):
            v = hist[k]
            for j in range(1, props + 1):
                v = jnp.where(picks[j], hist[j + k], v)
            win.append(v)
        win += rows_fresh
        for m, v in enumerate(win):
            out_ref[m, :, lo : lo + CHUNK] = v.astype(jnp.bfloat16)
        taps = [tap_ref[j : j + 1, lo : lo + CHUNK].astype(jnp.float32) for j in range(tap_ref.shape[0])]
        out = []
        for t in range(props):
            v = win[t] * taps[0]
            for j in range(1, len(taps)):
                v = v + win[t + j] * taps[j]
            out.append(silu(v))
        return out

    dt_raw = (head_part * scale).astype(jnp.bfloat16)
    dtw_wide = dot(dt_raw, expand.astype(jnp.bfloat16))
    head_lane = lax.broadcasted_iota(jnp.int32, (rows, 128), 1)
    raw = jnp.where(head_lane < heads, dt_raw.astype(jnp.float32), 0.0)
    a_ref[...] = jnp.exp(-jnp.exp(par[1:2]) * softplus(raw + par[0:1]))

    b_terms, c_low, pairs = [], [], []
    for j in range(n_chunk):
        bc = conv(bch_ref, bck_ref, bcwin_ref, fresh(j), j * CHUNK)
        for i in range(CHUNK // (2 * state)):
            b = [v[:, 2 * i * state : (2 * i + 1) * state] for v in bc]
            c = [v[:, (2 * i + 1) * state : (2 * i + 2) * state] for v in bc]
            g = len(c_low)
            b_ref[:, g * state : (g + 1) * state] = jnp.concatenate(b, axis=0).astype(jnp.bfloat16)
            c_low.append(jnp.concatenate(c, axis=0).astype(jnp.bfloat16))
            pairs.append({
                (t, r): jnp.broadcast_to(jnp.sum(c[t] * b[r], axis=1, keepdims=True), (seqs, span))
                for t in range(props) for r in range(t + 1)})

    carried = [jnp.zeros((rows, span), jnp.float32) for _ in range(groups)]
    for s in range(seqs):
        saved_copies[s].wait()
        s0 = saved[s][acc_smem[s]]
        s0_ref[s] = s0
        low = s0.reshape(heads * size, state).astype(jnp.bfloat16)
        for g in range(groups):
            masked = jnp.where(row % seqs == s, c_low[g].astype(jnp.float32), 0.0).astype(jnp.bfloat16)
            carried[g] = carried[g] + dot(masked, low[g * span : (g + 1) * span], NT)

    outs, gated_parts = [], []
    for j in range(n_chunk):
        lo = j * CHUNK
        sl = slice(lo, lo + CHUNK)
        xc = conv(xh_ref, xk_ref, xwin_ref, fresh(n_chunk + j), lo)
        sizes = [
            softplus(dtw_wide[t * seqs : (t + 1) * seqs, sl] + bias[:, sl]) for t in range(props)]
        xdt = [xc[t] * sizes[t] for t in range(props)]
        xdt_ref[:, sl] = jnp.concatenate(xdt, axis=0).astype(jnp.bfloat16)
        decays = [-rate[:, sl] * v for v in sizes]
        out_t = []
        for t in range(props):
            gap = decays[t]
            out = skip[:, sl] * xc[t]
            for r in range(t, -1, -1):
                pair = jnp.concatenate(
                    [pairs[j * in_chunk + i][(t, r)] for i in range(in_chunk)], axis=1)
                if r == t:
                    out = out + pair * xdt[r]
                else:
                    out = out + jnp.exp(gap) * pair * xdt[r]
                    gap = gap + decays[r]
            held = jnp.concatenate(
                [carried[j * in_chunk + i][t * seqs : (t + 1) * seqs] for i in range(in_chunk)], axis=1)
            out_t.append(out + jnp.exp(gap) * held)
        outs.append(out_t)
    square_sums = [jnp.zeros((seqs, 1), jnp.float32) for _ in range(props)]
    gain = gain_ref[...].astype(jnp.float32).reshape(1, inner)
    for j in range(n_chunk):
        sl = slice(j * CHUNK, (j + 1) * CHUNK)
        zs = fresh(2 * n_chunk + j)
        scaled_t = []
        for t in range(props):
            v = outs[j][t] * silu(zs[t])
            square_sums[t] = square_sums[t] + jnp.sum(v * v, axis=1, keepdims=True)
            scaled_t.append((v * gain[:, sl]).astype(jnp.bfloat16))
        gated_parts.append(jnp.concatenate(scaled_t, axis=0))
    scaled = jnp.concatenate(gated_parts, axis=1)

    diagonal = lax.broadcasted_iota(jnp.int32, (rows, 128), 0) == lax.broadcasted_iota(
        jnp.int32, (rows, 128), 1)
    norm_row = jnp.sum(
        jnp.where(diagonal, jnp.concatenate(square_sums, axis=0), 0.0), axis=0, keepdims=True)
    norm_out[...] = norm_row
    n_copies = [
        remote(norm_out, norm_in.at[i], n_send.at[i], n_recv.at[i], {"kv": p})
        for i, p in enumerate(exits)]
    for copy in n_copies:
        copy.start()
    o_copies = [
        remote(part.at[i], slots.at[i], o_send.at[i], o_recv.at[i], {"kv": p})
        for i, p in enumerate(exits)]
    for i in range(n_kv):
        ow_copies[i].wait()
        value = dot(scaled, w_buf[i])
        if i < n_kv - 1:
            part[i] = value.astype(jnp.bfloat16)
            o_copies[i].start()
    for copy in n_copies:
        copy.wait_recv()
    for i in range(n_kv - 1):
        norm_row = norm_row + norm_in[i]
    norm = lax.rsqrt(
        jnp.sum(jnp.where(diagonal, norm_row, 0.0), axis=1, keepdims=True) / channels + EPSILON)
    for i in range(n_kv - 2, -1, -1):
        o_copies[i].wait_recv()
        value = value + slots[i].astype(jnp.float32)
    value = value * norm
    for i in range(fin.shape[0]):
        for t in range(props):
            fin[i, pl.ds(t, seqs, stride=props), :] = value[
                t * seqs : (t + 1) * seqs, i * lanes : (i + 1) * lanes]
        mixed_ref[:, i * lanes : (i + 1) * lanes] = fin[i].astype(mixed_ref.dtype)
    for k in range(-1, n_big):
        core_copy(k).wait_send()
        x_copy(k).wait_send()
    for copy in n_copies + o_copies:
        copy.wait_send()


def write_kernel(
    mixed_ref, s0_ref, xdt_ref, b_ref, a_ref, xwin_ref, bcwin_ref,
    mixed_out, states_out, xwin_out, bcwin_out,
    a_smem, new, a_sem, small_sem, first_sem, new_sem,
):
    seqs, heads, size, state = s0_ref.shape
    rows = b_ref.shape[0]
    props = rows // seqs
    groups = b_ref.shape[1] // state
    per = heads // groups
    span = per * size
    a_copy = pltpu.make_async_copy(a_ref, a_smem, a_sem)
    a_copy.start()
    copies = [
        pltpu.make_async_copy(s0_ref.at[s], states_out.at[s, 0], first_sem.at[s]) for s in range(seqs)]
    copies += [
        pltpu.make_async_copy(src, dst, small_sem.at[i])
        for i, (src, dst) in enumerate(
            [(mixed_ref, mixed_out), (xwin_ref, xwin_out), (bcwin_ref, bcwin_out)])]
    for copy in copies:
        copy.start()
    row = lax.broadcasted_iota(jnp.int32, (rows, state), 0)
    a_copy.wait()
    turned = [
        jnp.transpose(xdt_ref[:, g * span : (g + 1) * span].astype(jnp.float32)).astype(jnp.bfloat16)
        for g in range(groups)]

    def new_copy(s):
        return pltpu.make_async_copy(
            new.at[s], states_out.at[s, pl.ds(1, props)], new_sem.at[s])

    for s in range(seqs):
        for g in range(groups):
            b = b_ref[:, g * state : (g + 1) * state].astype(jnp.float32)
            masked = jnp.concatenate(
                [jnp.where(row == t * seqs + s, b, 0.0) for t in range(props)],
                axis=1).astype(jnp.bfloat16)
            outer = dot(turned[g], masked)
            for h in range(per):
                head = g * per + h
                now = s0_ref[s, head]
                for t in range(props):
                    now = a_smem[t * seqs + s, head] * now + outer[
                        h * size : (h + 1) * size, t * state : (t + 1) * state]
                    new[s, t, head] = now
        new_copy(s).start()
    for copy in copies:
        copy.wait()
    for s in range(seqs):
        new_copy(s).wait()


def local(
    hidden, input_gain, x_weight, z_weight, bc_weight, dt_weight, x_kernel, bc_kernel,
    dt_bias, decay_log, skip_scale, output_gain, output_weight, saved_states,
    x_history, bc_history, accepted,
):
    heads = dt_bias.shape[0]
    seqs, kept, _, size, state = saved_states.shape
    hist = x_history.shape[1]
    tokens, depth = hidden.shape
    inner, bcw = x_weight.shape[1], bc_weight.shape[1]
    n_kv, n_tp = lax.axis_size("kv"), lax.axis_size("tp")
    rows = tokens // n_tp
    props = rows // seqs
    block = output_weight.shape[1] // n_kv
    n_big = 3 * inner // CHUNK
    f32, bf16 = jnp.float32, jnp.bfloat16

    vmem = pl.BlockSpec(memory_space=pltpu.VMEM)
    anym = pl.BlockSpec(memory_space=pl.ANY)
    smem = pl.BlockSpec(memory_space=pltpu.SMEM)
    dma = pltpu.SemaphoreType.DMA
    shapes = (
        ((rows, block), bf16), ((seqs, heads, size, state), f32), ((rows, inner), bf16),
        ((rows, bcw // 2), bf16), ((rows, 128), f32), ((hist, seqs, inner), bf16),
        ((hist, seqs, bcw), bf16))
    middle = pl.pallas_call(
        functools.partial(main_kernel, depth * n_tp, inner * n_kv, n_kv),
        out_shape=tuple(pltpu.VMEM(*s) for s in shapes),
        in_specs=[smem] * 4 + [anym, vmem] + [anym] * 4 + [vmem] * 5 + [anym] * 2,
        out_specs=[vmem] * len(shapes),
        scratch_shapes=[
            pltpu.VMEM((tokens, depth), bf16),
            pltpu.VMEM((depth // 128, tokens, 128), f32),
            pltpu.VMEM((128, depth), bf16),
            pltpu.VMEM((n_big, depth, CHUNK), bf16),
            pltpu.VMEM((n_tp, rows, 128), bf16),
            pltpu.VMEM((n_big, n_tp, rows, CHUNK), bf16),
            pltpu.VMEM((2, rows, 128), bf16),
            pltpu.VMEM((n_big, 2, rows, CHUNK), bf16),
            pltpu.VMEM((rows, 128), bf16),
            pltpu.VMEM((n_big, rows, CHUNK), bf16),
            pltpu.VMEM((rows, 128), f32),
            pltpu.VMEM((n_big, rows, CHUNK), f32),
            pltpu.VMEM((rows, 128), bf16),
            pltpu.VMEM((n_big, rows, CHUNK), bf16),
            pltpu.VMEM((n_kv, inner, block), bf16),
            pltpu.VMEM((n_kv - 1, rows, block), bf16),
            pltpu.VMEM((n_kv - 1, rows, block), bf16),
            pltpu.VMEM((1, 128), f32),
            pltpu.VMEM((n_kv - 1, 1, 128), f32),
            pltpu.VMEM((block // 128, rows, 128), f32),
            dma((2,)), dma((n_big,)), dma((seqs,)), dma((n_kv,)),
            dma((n_big + 1,)), dma((n_big + 1,)), dma((n_big + 1,)), dma((n_big + 1,)),
            dma((n_kv - 1,)), dma((n_kv - 1,)), dma((n_kv - 1,)), dma((n_kv - 1,)),
        ] + [pltpu.VMEM((kept, heads, size, state), f32)] * seqs,
        compiler_params=pltpu.CompilerParams(
            vmem_limit_bytes=48 << 20, collective_id=0, has_side_effects=True),
        cost_estimate=pl.CostEstimate(
            flops=2 * tokens * depth * 3 * inner, bytes_accessed=36 << 20, transcendentals=0),
        name="mixer",
    )(
        accepted, dt_bias, decay_log, skip_scale,
        hidden, input_gain, x_weight, z_weight, bc_weight, dt_weight.T,
        x_history.transpose(1, 0, 2), bc_history.transpose(1, 0, 2),
        x_kernel, bc_kernel, output_gain, saved_states, output_weight,
    )
    mixed, new_states, xw, bcw_out = pl.pallas_call(
        write_kernel,
        out_shape=(
            jax.ShapeDtypeStruct((rows, block), bf16),
            jax.ShapeDtypeStruct(saved_states.shape, f32),
            jax.ShapeDtypeStruct((hist, seqs, inner), bf16),
            jax.ShapeDtypeStruct((hist, seqs, bcw), bf16)),
        in_specs=[vmem] * len(shapes),
        out_specs=[anym] * 4,
        scratch_shapes=[
            pltpu.SMEM((rows, 128), f32),
            pltpu.VMEM((seqs, props, heads, size, state), f32),
            dma, dma((3,)), dma((seqs,)), dma((seqs,)),
        ],
        compiler_params=pltpu.CompilerParams(vmem_limit_bytes=32 << 20),
        cost_estimate=pl.CostEstimate(
            flops=2 * saved_states.size, bytes_accessed=6 * saved_states.size, transcendentals=0),
        name="write",
    )(*[pltpu.with_memory_space_constraint(v, pltpu.VMEM) for v in middle])
    return (mixed, new_states, xw.transpose(1, 0, 2), bcw_out.transpose(1, 0, 2))


def fits(mesh):
    n_kv, n_tp = mesh.shape["kv"], mesh.shape["tp"]
    inner = INNER // n_kv
    return inner % 1024 == 0 and n_kv > 1 and n_kv & (n_kv - 1) == 0 and n_tp == 4


def solution(mesh):
    in_specs = (
        P(None, "tp"),
        P("tp"),
        P("tp", "kv"),
        P("tp", "kv"),
        P("tp", "kv"),
        P("tp", "kv"),
        P(None, "kv"),
        P(None, "kv"),
        P("kv"),
        P("kv"),
        P("kv"),
        P("kv"),
        P("kv", None),
        P("tp", None, "kv", None, None),
        P("tp", None, "kv"),
        P("tp", None, "kv"),
        P("tp"),
    )
    out_specs = (
        P("tp", "kv"),
        P("tp", None, "kv", None, None),
        P("tp", None, "kv"),
        P("tp", None, "kv"),
    )
    body = local if fits(mesh) else local_general
    return jax.shard_map(body, mesh=mesh, in_specs=in_specs, out_specs=out_specs, check_vma=False)
```

```python
import jax
import jax.numpy as jnp
import functools

from jax import lax
from jax.experimental import pallas as pl
from jax.experimental.pallas import tpu as pltpu
from jax.sharding import PartitionSpec as P

D = 4096
PROPS = 4
INNER = 8192


EPSILON = 1e-05


def partner_2(block, axis, stride):
    count = lax.axis_size(axis)
    route = []
    for low in range(count):
        high = low | 1 << stride
        if high != low and high < count:
            route += [(low, high), (high, low)]
    return lax.ppermute(block, axis, route)


def take_window(history, accepted, fresh_rows):
    history_len = history.shape[1] - fresh_rows.shape[1]
    indices = accepted[:, None] + jnp.arange(history_len, dtype=jnp.int32)[None, :]
    kept_rows = jnp.take_along_axis(history, indices[:, :, None], axis=1)
    return jnp.concatenate([kept_rows, fresh_rows], axis=1)


def conv_silu(window, kernel):
    length = window.shape[1] - kernel.shape[0] + 1
    running = window[:, 0:length].astype(jnp.float32) * kernel[0].astype(jnp.float32)
    for offset in range(1, kernel.shape[0]):
        running = running + window[:, offset : offset + length].astype(jnp.float32) * kernel[
            offset
        ].astype(jnp.float32)
    return jax.nn.silu(running)


def ssd_block(x_conv, step_size, decay_rate, b_terms, c_terms, first_state, skip_scale):
    cumulated = jnp.cumsum(-decay_rate * step_size, axis=1)
    length = x_conv.shape[1]
    indices = jnp.arange(length)
    causal = indices[:, None] >= indices[None, :]
    gaps = cumulated[:, :, None, :] - cumulated[:, None, :, :]
    weights = jnp.exp(jnp.where(causal[None, :, :, None], gaps, -jnp.inf))
    inputs = x_conv * step_size[..., None]
    outer_prod = jnp.einsum("srhp,srhn->srhpn", inputs, b_terms)
    states = jnp.exp(cumulated)[..., None, None] * first_state[:, None] + jnp.einsum(
        "strh,srhpn->sthpn", weights, outer_prod
    )
    output = jnp.einsum("sthn,sthpn->sthp", c_terms, states) + skip_scale[:, None] * x_conv
    return (output, states)


def local_general(
    hidden,
    input_gain,
    x_weight,
    z_weight,
    bc_weight,
    dt_weight,
    x_kernel,
    bc_kernel,
    dt_bias,
    decay_log,
    skip_scale,
    output_gain,
    output_weight,
    saved_states,
    x_history,
    bc_history,
    accepted,
):
    heads_here = dt_bias.shape[0]
    head_size = x_weight.shape[1] // heads_here
    state_size = saved_states.shape[4]
    seqs_here = accepted.shape[0]
    rows_here = hidden.shape[0] // lax.axis_size("tp")
    inner_here = x_weight.shape[1]
    bc_here = bc_weight.shape[1]
    widened = hidden.astype(jnp.float32)
    squares = lax.psum(jnp.sum(widened * widened, axis=1), "tp")
    normed = (
        widened * lax.rsqrt(squares[:, None] / D + EPSILON) * input_gain.astype(jnp.float32)
    ).astype(jnp.bfloat16)
    weights = jnp.concatenate([x_weight, z_weight, bc_weight, dt_weight], axis=1)
    product = jnp.dot(normed, weights, preferred_element_type=jnp.float32)
    projected = lax.psum_scatter(
        lax.optimization_barrier(product.astype(jnp.bfloat16))
        .astype(jnp.float32)
        .astype(jnp.bfloat16),
        "tp",
        scatter_dimension=0,
        tiled=True,
    )
    x_fresh = projected[:, :inner_here]
    z_fresh = projected[:, inner_here : 2 * inner_here]
    bc_fresh = projected[:, 2 * inner_here : 2 * inner_here + bc_here]
    dt_fresh = projected[:, 2 * inner_here + bc_here :]
    x_window = take_window(x_history, accepted, x_fresh.reshape(seqs_here, PROPS, inner_here))
    bc_window = take_window(bc_history, accepted, bc_fresh.reshape(seqs_here, PROPS, bc_here))
    x_conv = conv_silu(x_window, x_kernel).reshape(seqs_here, PROPS, heads_here, head_size)
    bc_conv = conv_silu(bc_window, bc_kernel)
    spread = max(4 // heads_here, 1)
    position = lax.axis_index("kv")
    for level in range(spread.bit_length() - 1):
        partner = partner_2(bc_conv, "kv", level)
        low_half = position // 2**level % 2 == 0
        bc_conv = jnp.where(
            low_half,
            jnp.concatenate([bc_conv, partner], axis=2),
            jnp.concatenate([partner, bc_conv], axis=2),
        )
    groups_here = bc_conv.shape[2] // (2 * state_size)
    paired = bc_conv.reshape(seqs_here, PROPS, groups_here, 2, state_size)
    per_group = heads_here // groups_here
    b_terms = jnp.repeat(paired[:, :, :, 0], per_group, axis=2)
    c_terms = jnp.repeat(paired[:, :, :, 1], per_group, axis=2)
    step_size = jax.nn.softplus(
        dt_fresh.astype(jnp.float32).reshape(seqs_here, PROPS, heads_here) + dt_bias
    )
    first_state = jnp.take_along_axis(saved_states, accepted[:, None, None, None, None], axis=1)[
        :, 0
    ]
    output, states = ssd_block(
        x_conv, step_size, jnp.exp(decay_log), b_terms, c_terms, first_state, skip_scale
    )
    new_states = jnp.concatenate([first_state[:, None], states], axis=1)
    gate_values = z_fresh.astype(jnp.float32).reshape(seqs_here, PROPS, heads_here, head_size)
    gated = (output * jax.nn.silu(gate_values)).reshape(rows_here, inner_here)
    square_sum = jnp.sum(gated * gated, axis=1)
    scaled = (gated * output_gain.astype(jnp.float32)).astype(jnp.bfloat16)
    partial_value = jnp.dot(scaled, output_weight, preferred_element_type=jnp.float32)
    total_squares = lax.psum(square_sum, "kv")
    summed = lax.psum_scatter(partial_value, "kv", scatter_dimension=1, tiled=True)
    mixed = (lax.rsqrt(total_squares / INNER + EPSILON)[:, None] * summed).astype(jnp.bfloat16)
    return (mixed, new_states, x_window, bc_window)


NN = (((1,), (0,)), ((), ()))
NT = (((1,), (1,)), ((), ()))
CHUNK = 512
LAG = 2
AHEAD = 4


def dot(a, b, dims=NN, **kw):
    return lax.dot_general(a, b, dims, preferred_element_type=jnp.float32, **kw)


def silu(v):
    return v / (1.0 + jnp.exp(-v))


def softplus(v):
    return jnp.maximum(v, 0.0) + jnp.log(1.0 + jnp.exp(-jnp.abs(v)))


def flip(index, mask):
    out = index
    bit = 1
    while bit <= mask:
        if mask & bit:
            out = out + bit - 2 * bit * lax.rem(index // bit, 2)
        bit *= 2
    return out


def remote(src, dst, send_sem, recv_sem, device):
    return pltpu.make_async_remote_copy(
        src_ref=src, dst_ref=dst, send_sem=send_sem, recv_sem=recv_sem,
        device_id=device, device_id_type=pl.DeviceIdType.MESH)


def main_kernel(
    features, channels, n_kv,
    acc_hbm, bias_hbm, decay_hbm, skip_hbm,
    hid_hbm, gin_hbm, xw_hbm, zw_hbm, bcw_hbm, dtw_hbm, xh_hbm, bch_hbm, xk_hbm, bck_hbm, gain_hbm,
    saved_hbm, w_hbm,
    mixed_ref, s0_ref, xdt_ref, b_ref, a_ref, xwin_ref, bcwin_ref,
    acc_smem, bias_smem, decay_smem, skip_smem, gin_ref, xh_ref, bch_ref, xk_ref, bck_ref, gain_ref,
    hid, entry32, dtw, wbuf, prod_dt, prod, peer_dt, peer, half_dt, half, own_dt, own, far_dt, far,
    w_buf, part, slots, norm_out, norm_in, fin,
    hid_sem, small_sem, w_sem, saved_sem, ow_sem, c_send, c_recv, x_send, x_recv, o_send, o_recv, n_send, n_recv,
    *saved,
):
    seqs = acc_smem.shape[0]
    rows = mixed_ref.shape[0]
    props = rows // seqs
    tokens = hid.shape[0]
    inner = xwin_ref.shape[2]
    _, heads, size, state = saved[0].shape
    groups = bcwin_ref.shape[2] // (2 * state)
    per = heads // groups
    span = per * size
    n_chunk = inner // CHUNK
    in_chunk = CHUNK // span
    block = mixed_ref.shape[1]

    kv, tp = lax.axis_index("kv"), lax.axis_index("tp")
    side, core = tp // 2, lax.rem(tp, 2)
    core_peer, x_peer = flip(tp, 1), flip(tp, 2)
    ranks = list(range(0, n_kv - 1, 2))
    ranks = ranks[: len(ranks) // 2] + ranks[: len(ranks) // 2 - 1 : -1] + list(range(1, n_kv - 1, 2))
    exits = [i + (i - kv + n_kv) // n_kv for i in ranks]

    barrier = pltpu.get_barrier_semaphore()
    for device in [{"tp": core_peer}, {"tp": x_peer}] + [{"kv": p} for p in exits]:
        pl.semaphore_signal(barrier, inc=1, device_id=device, device_id_type=pl.DeviceIdType.MESH)

    hid_copy = pltpu.make_async_copy(hid_hbm, hid, hid_sem.at[0])
    hid_copy.start()
    gin_copy = pltpu.make_async_copy(gin_hbm, gin_ref, hid_sem.at[1])
    gin_copy.start()
    dtw_copy = pltpu.make_async_copy(dtw_hbm, dtw.at[pl.ds(0, heads)], hid_sem.at[2])
    dtw_copy.start()
    w_copies = [
        pltpu.make_async_copy(src.at[:, pl.ds(j * CHUNK, CHUNK)], wbuf.at[i], w_sem.at[i])
        for i, (src, j) in enumerate(
            [(src, j) for src in (bcw_hbm, xw_hbm, zw_hbm) for j in range(n_chunk)])
    ]
    for copy in w_copies:
        copy.start()
    small_copies = [
        pltpu.make_async_copy(src, dst, small_sem.at[i])
        for i, (src, dst) in enumerate([
            (acc_hbm, acc_smem), (bias_hbm, bias_smem), (decay_hbm, decay_smem), (skip_hbm, skip_smem),
            (xh_hbm, xh_ref), (bch_hbm, bch_ref), (xk_hbm, xk_ref), (bck_hbm, bck_ref),
            (gain_hbm, gain_ref)])]
    for copy in small_copies:
        copy.start()
    n_big = len(w_copies)

    dtw[heads:] = jnp.zeros((dtw.shape[0] - heads, dtw.shape[1]), dtw.dtype)
    hid_copy.wait()
    lanes = entry32.shape[2]
    for i in range(entry32.shape[0]):
        entry32[i] = hid[:, i * lanes : (i + 1) * lanes].astype(jnp.float32)
    gin_copy.wait()
    gin = gin_ref[...].astype(jnp.float32).reshape(1, -1)
    entry, squares = [], []
    for p in range(tokens // rows):
        for t in range(props):
            v = jnp.concatenate(
                [entry32[i, pl.ds(p * rows + t, seqs, stride=props), :] for i in range(entry32.shape[0])],
                axis=1)
            squares.append(jnp.sum(v * v, axis=1, keepdims=True))
            entry.append(v * gin)
    entry = jnp.concatenate(entry, axis=0).astype(jnp.bfloat16)
    squares = jnp.concatenate(squares, axis=0)
    high = squares.astype(jnp.bfloat16).astype(jnp.float32)

    saved_copies = [
        pltpu.make_async_copy(saved_hbm.at[s], saved[s], saved_sem.at[s]) for s in range(seqs)]
    ow_copies = [
        pltpu.make_async_copy(
            w_hbm.at[:, pl.ds(pl.multiple_of(p * block, block), block)], w_buf.at[i], ow_sem.at[i])
        for i, p in enumerate(exits + [kv])]

    def put(ref, value):
        for p in range(tokens // rows):
            ref[(p % 2) * 2 + p // 2] = value[p * rows : (p + 1) * rows].astype(jnp.bfloat16)

    def core_copy(k):
        src, dst = (prod_dt, peer_dt) if k < 0 else (prod.at[k], peer.at[k])
        return remote(
            src.at[pl.ds(2 - 2 * core, 2)], dst, c_send.at[k + 1], c_recv.at[k + 1], {"tp": core_peer})

    def x_copy(k):
        src, dst = (half_dt, far_dt) if k < 0 else (half.at[k], far.at[k])
        return remote(src, dst, x_send.at[k + 1], x_recv.at[k + 1], {"tp": x_peer})

    def forward(k):
        core_copy(k).wait_recv()
        mine, theirs, send, keep = (prod_dt, peer_dt, half_dt, own_dt) if k < 0 else (
            prod.at[k], peer.at[k], half.at[k], own.at[k])
        away = mine[2 * core + 1 - side].astype(jnp.float32) + theirs[1 - side].astype(jnp.float32)
        send[...] = away.astype(jnp.bfloat16)
        x_copy(k).start()
        keep[...] = mine[2 * core + side].astype(jnp.float32) + theirs[side].astype(jnp.float32)

    dtw_copy.wait()
    lane = lax.broadcasted_iota(jnp.int32, (tokens, 128), 1)
    first = dot(entry, dtw[...], NT)
    first = jnp.where(lane == 126, high, jnp.where(lane == 127, squares - high, first))
    put(prod_dt, first)
    pl.semaphore_wait(barrier, 2 + len(exits))
    core_copy(-1).start()
    for k in range(n_big):
        w_copies[k].wait()
        put(prod.at[k], dot(entry, wbuf[k]))
        core_copy(k).start()
        if k >= LAG - 1:
            forward(k - LAG)
        if k == 0:
            for copy in saved_copies:
                copy.start()
    for k in range(n_big - LAG, n_big):
        forward(k)

    for copy in small_copies:
        copy.wait()
    seq_at = lax.broadcasted_iota(jnp.int32, (seqs, CHUNK), 0)
    acc = jnp.zeros((seqs, CHUNK), jnp.int32)
    for s in range(seqs):
        acc = jnp.where(seq_at == s, acc_smem[s], acc)
    picks = [acc == j for j in range(props + 1)]
    eh = lax.broadcasted_iota(jnp.int32, (128, inner), 0)
    ec = lax.broadcasted_iota(jnp.int32, (128, inner), 1)
    expand = (eh == ec // size).astype(jnp.float32)
    lane_at = lax.broadcasted_iota(jnp.int32, (8, 128), 1)
    row_at = lax.broadcasted_iota(jnp.int32, (8, 128), 0)
    par = jnp.zeros((8, 128), jnp.float32)
    for i, smem in enumerate((bias_smem, decay_smem, skip_smem)):
        for h in range(heads):
            par = jnp.where((row_at == i) & (lane_at == h), smem[h], par)
    wide = dot(par, expand, precision=lax.Precision.HIGHEST)
    bias, rate, skip = wide[0:1], jnp.exp(wide[1:2]), wide[2:3]
    row = lax.broadcasted_iota(jnp.int32, (rows, state), 0)

    def total(k):
        x_copy(k).wait_recv()
        if k < 0:
            return own_dt[...] + far_dt[...].astype(jnp.float32)
        return own[k] + far[k].astype(jnp.float32)

    head_part = total(-1)
    sums = head_part[:, 126:127] + head_part[:, 127:128]
    scale = lax.rsqrt(sums / features + EPSILON)

    def fresh(k):
        v = (total(k) * scale).astype(jnp.bfloat16).astype(jnp.float32)
        return [v[t * seqs : (t + 1) * seqs] for t in range(props)]

    def conv(hist_ref, tap_ref, out_ref, rows_fresh, lo):
        kept = hist_ref.shape[0] - props
        hist = [hist_ref[m, :, lo : lo + CHUNK].astype(jnp.float32) for m in range(hist_ref.shape[0])]
        win = []
        for k in range(kept):
            v = hist[k]
            for j in range(1, props + 1):
                v = jnp.where(picks[j], hist[j + k], v)
            win.append(v)
        win += rows_fresh
        for m, v in enumerate(win):
            out_ref[m, :, lo : lo + CHUNK] = v.astype(jnp.bfloat16)
        taps = [tap_ref[j : j + 1, lo : lo + CHUNK].astype(jnp.float32) for j in range(tap_ref.shape[0])]
        out = []
        for t in range(props):
            v = win[t] * taps[0]
            for j in range(1, len(taps)):
                v = v + win[t + j] * taps[j]
            out.append(silu(v))
        return out

    dt_raw = (head_part * scale).astype(jnp.bfloat16)
    dtw_wide = dot(dt_raw, expand.astype(jnp.bfloat16))
    head_lane = lax.broadcasted_iota(jnp.int32, (rows, 128), 1)
    raw = jnp.where(head_lane < heads, dt_raw.astype(jnp.float32), 0.0)
    a_ref[...] = jnp.exp(-jnp.exp(par[1:2]) * softplus(raw + par[0:1]))

    b_terms, c_low, pairs = [], [], []
    for j in range(n_chunk):
        bc = conv(bch_ref, bck_ref, bcwin_ref, fresh(j), j * CHUNK)
        for i in range(CHUNK // (2 * state)):
            b = [v[:, 2 * i * state : (2 * i + 1) * state] for v in bc]
            c = [v[:, (2 * i + 1) * state : (2 * i + 2) * state] for v in bc]
            g = len(c_low)
            b_ref[:, g * state : (g + 1) * state] = jnp.concatenate(b, axis=0).astype(jnp.bfloat16)
            c_low.append(jnp.concatenate(c, axis=0).astype(jnp.bfloat16))
            pairs.append({
                (t, r): jnp.broadcast_to(jnp.sum(c[t] * b[r], axis=1, keepdims=True), (seqs, span))
                for t in range(props) for r in range(t + 1)})

    outs, gated_parts = [], []
    for j in range(n_chunk):
        lo = j * CHUNK
        sl = slice(lo, lo + CHUNK)
        xc = conv(xh_ref, xk_ref, xwin_ref, fresh(n_chunk + j), lo)
        sizes = [
            softplus(dtw_wide[t * seqs : (t + 1) * seqs, sl] + bias[:, sl]) for t in range(props)]
        xdt = [xc[t] * sizes[t] for t in range(props)]
        xdt_ref[:, sl] = jnp.concatenate(xdt, axis=0).astype(jnp.bfloat16)
        decays = [-rate[:, sl] * v for v in sizes]
        out_t = []
        for t in range(props):
            gap = decays[t]
            out = skip[:, sl] * xc[t]
            for r in range(t, -1, -1):
                pair = jnp.concatenate(
                    [pairs[j * in_chunk + i][(t, r)] for i in range(in_chunk)], axis=1)
                if r == t:
                    out = out + pair * xdt[r]
                else:
                    out = out + jnp.exp(gap) * pair * xdt[r]
                    gap = gap + decays[r]
            out_t.append((out, jnp.exp(gap)))
        outs.append(out_t)

    carried = [jnp.zeros((rows, span), jnp.float32) for _ in range(groups)]
    for s in range(seqs):
        saved_copies[s].wait()
        if s == seqs - AHEAD:
            for copy in ow_copies:
                copy.start()
        s0 = saved[s][acc_smem[s]]
        s0_ref[s] = s0
        low = s0.reshape(heads * size, state).astype(jnp.bfloat16)
        for g in range(groups):
            masked = jnp.where(row % seqs == s, c_low[g].astype(jnp.float32), 0.0).astype(jnp.bfloat16)
            carried[g] = carried[g] + dot(masked, low[g * span : (g + 1) * span], NT)

    square_sums = [jnp.zeros((seqs, 1), jnp.float32) for _ in range(props)]
    gain = gain_ref[...].astype(jnp.float32).reshape(1, inner)
    for j in range(n_chunk):
        sl = slice(j * CHUNK, (j + 1) * CHUNK)
        zs = fresh(2 * n_chunk + j)
        scaled_t = []
        for t in range(props):
            held = jnp.concatenate(
                [carried[j * in_chunk + i][t * seqs : (t + 1) * seqs] for i in range(in_chunk)], axis=1)
            out, fade = outs[j][t]
            v = (out + fade * held) * silu(zs[t])
            square_sums[t] = square_sums[t] + jnp.sum(v * v, axis=1, keepdims=True)
            scaled_t.append((v * gain[:, sl]).astype(jnp.bfloat16))
        gated_parts.append(jnp.concatenate(scaled_t, axis=0))
    scaled = jnp.concatenate(gated_parts, axis=1)

    diagonal = lax.broadcasted_iota(jnp.int32, (rows, 128), 0) == lax.broadcasted_iota(
        jnp.int32, (rows, 128), 1)
    norm_row = jnp.sum(
        jnp.where(diagonal, jnp.concatenate(square_sums, axis=0), 0.0), axis=0, keepdims=True)
    norm_out[...] = norm_row
    n_copies = [
        remote(norm_out, norm_in.at[kv], n_send.at[i], n_recv.at[kv], {"kv": p})
        for i, p in enumerate(exits)]
    for copy in n_copies:
        copy.start()
    o_copies = [
        remote(part.at[i], slots.at[kv], o_send.at[i], o_recv.at[kv], {"kv": p})
        for i, p in enumerate(exits)]
    sources = [flip(kv, d) for d in range(1, n_kv)]

    def arrived(p):
        remote(norm_out, norm_in.at[p], n_send.at[0], n_recv.at[p], {"kv": p}).wait_recv()

    def landed(p):
        remote(part.at[0], slots.at[p], o_send.at[0], o_recv.at[p], {"kv": p}).wait_recv()

    for i in range(n_kv):
        ow_copies[i].wait()
        value = dot(scaled, w_buf[i])
        if i < n_kv - 1:
            part[i] = value.astype(jnp.bfloat16)
            o_copies[i].start()
    for p in sources:
        arrived(p)
        norm_row = norm_row + norm_in[p]
    norm = lax.rsqrt(
        jnp.sum(jnp.where(diagonal, norm_row, 0.0), axis=1, keepdims=True) / channels + EPSILON)
    for p in sources:
        landed(p)
        value = value + slots[p].astype(jnp.float32)
    value = value * norm
    for i in range(fin.shape[0]):
        for t in range(props):
            fin[i, pl.ds(t, seqs, stride=props), :] = value[
                t * seqs : (t + 1) * seqs, i * lanes : (i + 1) * lanes]
        mixed_ref[:, i * lanes : (i + 1) * lanes] = fin[i].astype(mixed_ref.dtype)
    for k in range(-1, n_big):
        core_copy(k).wait_send()
        x_copy(k).wait_send()
    for copy in n_copies + o_copies:
        copy.wait_send()


def write_kernel(
    mixed_ref, s0_ref, xdt_ref, b_ref, a_ref, xwin_ref, bcwin_ref,
    mixed_out, states_out, xwin_out, bcwin_out,
    a_smem, new, a_sem, small_sem, first_sem, new_sem,
):
    seqs, heads, size, state = s0_ref.shape
    rows = b_ref.shape[0]
    props = rows // seqs
    groups = b_ref.shape[1] // state
    per = heads // groups
    span = per * size
    a_copy = pltpu.make_async_copy(a_ref, a_smem, a_sem)
    a_copy.start()
    copies = [
        pltpu.make_async_copy(s0_ref.at[s], states_out.at[s, 0], first_sem.at[s]) for s in range(seqs)]
    copies += [
        pltpu.make_async_copy(src, dst, small_sem.at[i])
        for i, (src, dst) in enumerate(
            [(mixed_ref, mixed_out), (xwin_ref, xwin_out), (bcwin_ref, bcwin_out)])]
    for copy in copies:
        copy.start()
    row = lax.broadcasted_iota(jnp.int32, (rows, state), 0)
    a_copy.wait()
    turned = [
        jnp.transpose(xdt_ref[:, g * span : (g + 1) * span].astype(jnp.float32)).astype(jnp.bfloat16)
        for g in range(groups)]

    def new_copy(s):
        return pltpu.make_async_copy(
            new.at[s], states_out.at[s, pl.ds(1, props)], new_sem.at[s])

    for s in range(seqs):
        for g in range(groups):
            b = b_ref[:, g * state : (g + 1) * state].astype(jnp.float32)
            masked = jnp.concatenate(
                [jnp.where(row == t * seqs + s, b, 0.0) for t in range(props)],
                axis=1).astype(jnp.bfloat16)
            outer = dot(turned[g], masked)
            for h in range(per):
                head = g * per + h
                now = s0_ref[s, head]
                for t in range(props):
                    now = a_smem[t * seqs + s, head] * now + outer[
                        h * size : (h + 1) * size, t * state : (t + 1) * state]
                    new[s, t, head] = now
        new_copy(s).start()
    for copy in copies:
        copy.wait()
    for s in range(seqs):
        new_copy(s).wait()


def local(
    hidden, input_gain, x_weight, z_weight, bc_weight, dt_weight, x_kernel, bc_kernel,
    dt_bias, decay_log, skip_scale, output_gain, output_weight, saved_states,
    x_history, bc_history, accepted,
):
    heads = dt_bias.shape[0]
    seqs, kept, _, size, state = saved_states.shape
    hist = x_history.shape[1]
    tokens, depth = hidden.shape
    inner, bcw = x_weight.shape[1], bc_weight.shape[1]
    n_kv, n_tp = lax.axis_size("kv"), lax.axis_size("tp")
    rows = tokens // n_tp
    props = rows // seqs
    block = output_weight.shape[1] // n_kv
    n_big = 3 * inner // CHUNK
    f32, bf16 = jnp.float32, jnp.bfloat16

    vmem = pl.BlockSpec(memory_space=pltpu.VMEM)
    anym = pl.BlockSpec(memory_space=pl.ANY)
    dma = pltpu.SemaphoreType.DMA
    shapes = (
        ((rows, block), bf16), ((seqs, heads, size, state), f32), ((rows, inner), bf16),
        ((rows, bcw // 2), bf16), ((rows, 128), f32), ((hist, seqs, inner), bf16),
        ((hist, seqs, bcw), bf16))
    middle = pl.pallas_call(
        functools.partial(main_kernel, depth * n_tp, inner * n_kv, n_kv),
        out_shape=tuple(pltpu.VMEM(*s) for s in shapes),
        in_specs=[pl.BlockSpec(memory_space=pltpu.HBM)] * 17,
        out_specs=[vmem] * len(shapes),
        scratch_shapes=[
            pltpu.SMEM((seqs,), jnp.int32),
            pltpu.SMEM((heads,), f32),
            pltpu.SMEM((heads,), f32),
            pltpu.SMEM((heads,), f32),
            pltpu.VMEM((depth,), bf16),
            pltpu.VMEM((hist, seqs, inner), bf16),
            pltpu.VMEM((hist, seqs, bcw), bf16),
            pltpu.VMEM(x_kernel.shape, bf16),
            pltpu.VMEM(bc_kernel.shape, bf16),
            pltpu.VMEM((inner,), bf16),
            pltpu.VMEM((tokens, depth), bf16),
            pltpu.VMEM((depth // 128, tokens, 128), f32),
            pltpu.VMEM((128, depth), bf16),
            pltpu.VMEM((n_big, depth, CHUNK), bf16),
            pltpu.VMEM((n_tp, rows, 128), bf16),
            pltpu.VMEM((n_big, n_tp, rows, CHUNK), bf16),
            pltpu.VMEM((2, rows, 128), bf16),
            pltpu.VMEM((n_big, 2, rows, CHUNK), bf16),
            pltpu.VMEM((rows, 128), bf16),
            pltpu.VMEM((n_big, rows, CHUNK), bf16),
            pltpu.VMEM((rows, 128), f32),
            pltpu.VMEM((n_big, rows, CHUNK), f32),
            pltpu.VMEM((rows, 128), bf16),
            pltpu.VMEM((n_big, rows, CHUNK), bf16),
            pltpu.VMEM((n_kv, inner, block), bf16),
            pltpu.VMEM((n_kv - 1, rows, block), bf16),
            pltpu.VMEM((n_kv, rows, block), bf16),
            pltpu.VMEM((1, 128), f32),
            pltpu.VMEM((n_kv, 1, 128), f32),
            pltpu.VMEM((block // 128, rows, 128), f32),
            dma((3,)), dma((9,)), dma((n_big,)), dma((seqs,)), dma((n_kv,)),
            dma((n_big + 1,)), dma((n_big + 1,)), dma((n_big + 1,)), dma((n_big + 1,)),
            dma((n_kv - 1,)), dma((n_kv,)), dma((n_kv - 1,)), dma((n_kv,)),
        ] + [pltpu.VMEM((kept, heads, size, state), f32)] * seqs,
        compiler_params=pltpu.CompilerParams(
            vmem_limit_bytes=48 << 20, collective_id=0, has_side_effects=True),
        cost_estimate=pl.CostEstimate(
            flops=2 * tokens * depth * 3 * inner, bytes_accessed=36 << 20, transcendentals=0),
        name="mixer",
    )(*[pltpu.with_memory_space_constraint(v, pltpu.HBM) for v in (
        accepted, dt_bias, decay_log, skip_scale,
        hidden, input_gain, x_weight, z_weight, bc_weight, dt_weight.T,
        x_history.transpose(1, 0, 2), bc_history.transpose(1, 0, 2),
        x_kernel, bc_kernel, output_gain, saved_states, output_weight,
    )])
    mixed, new_states, xw, bcw_out = pl.pallas_call(
        write_kernel,
        out_shape=(
            jax.ShapeDtypeStruct((rows, block), bf16),
            jax.ShapeDtypeStruct(saved_states.shape, f32),
            jax.ShapeDtypeStruct((hist, seqs, inner), bf16),
            jax.ShapeDtypeStruct((hist, seqs, bcw), bf16)),
        in_specs=[vmem] * len(shapes),
        out_specs=[anym] * 4,
        scratch_shapes=[
            pltpu.SMEM((rows, 128), f32),
            pltpu.VMEM((seqs, props, heads, size, state), f32),
            dma, dma((3,)), dma((seqs,)), dma((seqs,)),
        ],
        compiler_params=pltpu.CompilerParams(vmem_limit_bytes=32 << 20),
        cost_estimate=pl.CostEstimate(
            flops=2 * saved_states.size, bytes_accessed=6 * saved_states.size, transcendentals=0),
        name="write",
    )(*[pltpu.with_memory_space_constraint(v, pltpu.VMEM) for v in middle])
    return (mixed, new_states, xw.transpose(1, 0, 2), bcw_out.transpose(1, 0, 2))


def fits(mesh):
    n_kv, n_tp = mesh.shape["kv"], mesh.shape["tp"]
    inner = INNER // n_kv
    return inner % 1024 == 0 and n_kv > 1 and n_kv & (n_kv - 1) == 0 and n_tp == 4


def solution(mesh):
    in_specs = (
        P(None, "tp"),
        P("tp"),
        P("tp", "kv"),
        P("tp", "kv"),
        P("tp", "kv"),
        P("tp", "kv"),
        P(None, "kv"),
        P(None, "kv"),
        P("kv"),
        P("kv"),
        P("kv"),
        P("kv"),
        P("kv", None),
        P("tp", None, "kv", None, None),
        P("tp", None, "kv"),
        P("tp", None, "kv"),
        P("tp"),
    )
    out_specs = (
        P("tp", "kv"),
        P("tp", None, "kv", None, None),
        P("tp", None, "kv"),
        P("tp", None, "kv"),
    )
    body = local if fits(mesh) else local_general
    return jax.shard_map(body, mesh=mesh, in_specs=in_specs, out_specs=out_specs, check_vma=False)
```

```python
import jax
import jax.numpy as jnp
import functools

from jax import lax
from jax.experimental import pallas as pl
from jax.experimental.pallas import tpu as pltpu
from jax.sharding import PartitionSpec as P

D = 4096
PROPS = 4
INNER = 8192

EPSILON = 1e-05


def partner_2(block, axis, stride):
    count = lax.axis_size(axis)
    route = []
    for low in range(count):
        high = low | 1 << stride
        if high != low and high < count:
            route += [(low, high), (high, low)]
    return lax.ppermute(block, axis, route)


def take_window(history, accepted, fresh_rows):
    history_len = history.shape[1] - fresh_rows.shape[1]
    indices = accepted[:, None] + jnp.arange(history_len, dtype=jnp.int32)[None, :]
    kept_rows = jnp.take_along_axis(history, indices[:, :, None], axis=1)
    return jnp.concatenate([kept_rows, fresh_rows], axis=1)


def conv_silu(window, kernel):
    length = window.shape[1] - kernel.shape[0] + 1
    running = window[:, 0:length].astype(jnp.float32) * kernel[0].astype(jnp.float32)
    for offset in range(1, kernel.shape[0]):
        running = running + window[:, offset : offset + length].astype(jnp.float32) * kernel[
            offset
        ].astype(jnp.float32)
    return jax.nn.silu(running)


def ssd_block(x_conv, step_size, decay_rate, b_terms, c_terms, first_state, skip_scale):
    cumulated = jnp.cumsum(-decay_rate * step_size, axis=1)
    length = x_conv.shape[1]
    indices = jnp.arange(length)
    causal = indices[:, None] >= indices[None, :]
    gaps = cumulated[:, :, None, :] - cumulated[:, None, :, :]
    weights = jnp.exp(jnp.where(causal[None, :, :, None], gaps, -jnp.inf))
    inputs = x_conv * step_size[..., None]
    outer_prod = jnp.einsum("srhp,srhn->srhpn", inputs, b_terms)
    states = jnp.exp(cumulated)[..., None, None] * first_state[:, None] + jnp.einsum(
        "strh,srhpn->sthpn", weights, outer_prod
    )
    output = jnp.einsum("sthn,sthpn->sthp", c_terms, states) + skip_scale[:, None] * x_conv
    return (output, states)


def local_general(
    hidden,
    input_gain,
    x_weight,
    z_weight,
    bc_weight,
    dt_weight,
    x_kernel,
    bc_kernel,
    dt_bias,
    decay_log,
    skip_scale,
    output_gain,
    output_weight,
    saved_states,
    x_history,
    bc_history,
    accepted,
):
    heads_here = dt_bias.shape[0]
    head_size = x_weight.shape[1] // heads_here
    state_size = saved_states.shape[4]
    seqs_here = accepted.shape[0]
    rows_here = hidden.shape[0] // lax.axis_size("tp")
    inner_here = x_weight.shape[1]
    bc_here = bc_weight.shape[1]
    widened = hidden.astype(jnp.float32)
    squares = lax.psum(jnp.sum(widened * widened, axis=1), "tp")
    normed = (
        widened * lax.rsqrt(squares[:, None] / D + EPSILON) * input_gain.astype(jnp.float32)
    ).astype(jnp.bfloat16)
    weights = jnp.concatenate([x_weight, z_weight, bc_weight, dt_weight], axis=1)
    product = jnp.dot(normed, weights, preferred_element_type=jnp.float32)
    projected = lax.psum_scatter(
        lax.optimization_barrier(product.astype(jnp.bfloat16))
        .astype(jnp.float32)
        .astype(jnp.bfloat16),
        "tp",
        scatter_dimension=0,
        tiled=True,
    )
    x_fresh = projected[:, :inner_here]
    z_fresh = projected[:, inner_here : 2 * inner_here]
    bc_fresh = projected[:, 2 * inner_here : 2 * inner_here + bc_here]
    dt_fresh = projected[:, 2 * inner_here + bc_here :]
    x_window = take_window(x_history, accepted, x_fresh.reshape(seqs_here, PROPS, inner_here))
    bc_window = take_window(bc_history, accepted, bc_fresh.reshape(seqs_here, PROPS, bc_here))
    x_conv = conv_silu(x_window, x_kernel).reshape(seqs_here, PROPS, heads_here, head_size)
    bc_conv = conv_silu(bc_window, bc_kernel)
    spread = max(4 // heads_here, 1)
    position = lax.axis_index("kv")
    for level in range(spread.bit_length() - 1):
        partner = partner_2(bc_conv, "kv", level)
        low_half = position // 2**level % 2 == 0
        bc_conv = jnp.where(
            low_half,
            jnp.concatenate([bc_conv, partner], axis=2),
            jnp.concatenate([partner, bc_conv], axis=2),
        )
    groups_here = bc_conv.shape[2] // (2 * state_size)
    paired = bc_conv.reshape(seqs_here, PROPS, groups_here, 2, state_size)
    per_group = heads_here // groups_here
    b_terms = jnp.repeat(paired[:, :, :, 0], per_group, axis=2)
    c_terms = jnp.repeat(paired[:, :, :, 1], per_group, axis=2)
    step_size = jax.nn.softplus(
        dt_fresh.astype(jnp.float32).reshape(seqs_here, PROPS, heads_here) + dt_bias
    )
    first_state = jnp.take_along_axis(saved_states, accepted[:, None, None, None, None], axis=1)[
        :, 0
    ]
    output, states = ssd_block(
        x_conv, step_size, jnp.exp(decay_log), b_terms, c_terms, first_state, skip_scale
    )
    new_states = jnp.concatenate([first_state[:, None], states], axis=1)
    gate_values = z_fresh.astype(jnp.float32).reshape(seqs_here, PROPS, heads_here, head_size)
    gated = (output * jax.nn.silu(gate_values)).reshape(rows_here, inner_here)
    square_sum = jnp.sum(gated * gated, axis=1)
    scaled = (gated * output_gain.astype(jnp.float32)).astype(jnp.bfloat16)
    partial_value = jnp.dot(scaled, output_weight, preferred_element_type=jnp.float32)
    total_squares = lax.psum(square_sum, "kv")
    summed = lax.psum_scatter(partial_value, "kv", scatter_dimension=1, tiled=True)
    mixed = (lax.rsqrt(total_squares / INNER + EPSILON)[:, None] * summed).astype(jnp.bfloat16)
    return (mixed, new_states, x_window, bc_window)

NN = (((1,), (0,)), ((), ()))
NT = (((1,), (1,)), ((), ()))
CHUNK = 512
LAG = 2


def dot(a, b, dims=NN, **kw):
    return lax.dot_general(a, b, dims, preferred_element_type=jnp.float32, **kw)


def silu(v):
    return v / (1.0 + jnp.exp(-v))


def softplus(v):
    return jnp.maximum(v, 0.0) + jnp.log(1.0 + jnp.exp(-jnp.abs(v)))


def flip(index, mask):
    out = index
    bit = 1
    while bit <= mask:
        if mask & bit:
            out = out + bit - 2 * bit * lax.rem(index // bit, 2)
        bit *= 2
    return out


def remote(src, dst, send_sem, recv_sem, device):
    return pltpu.make_async_remote_copy(
        src_ref=src, dst_ref=dst, send_sem=send_sem, recv_sem=recv_sem,
        device_id=device, device_id_type=pl.DeviceIdType.MESH)


def main_kernel(
    features, channels, n_kv,
    acc_hbm, bias_hbm, decay_hbm, skip_hbm,
    hid_hbm, gin_hbm, xw_hbm, zw_hbm, bcw_hbm, dtw_hbm, xh_hbm, bch_hbm, xk_hbm, bck_hbm, gain_hbm,
    saved_hbm, w_hbm,
    mixed_ref, s0_ref, xdt_ref, b_ref, a_ref, xwin_ref, bcwin_ref,
    acc_smem, bias_smem, decay_smem, skip_smem, gin_ref, xh_ref, bch_ref, xk_ref, bck_ref, gain_ref,
    hid, entry32, dtw, wbuf, prod_dt, prod, peer_dt, peer, half_dt, half, own_dt, own, far_dt, far,
    w_buf, part, slots, norm_out, norm_in, fin,
    hid_sem, small_sem, w_sem, saved_sem, ow_sem, c_send, c_recv, x_send, x_recv, o_send, o_recv, n_send, n_recv,
    *saved,
):
    seqs = acc_smem.shape[0]
    rows = mixed_ref.shape[0]
    props = rows // seqs
    tokens = hid.shape[0]
    inner = xwin_ref.shape[2]
    _, heads, size, state = saved[0].shape
    groups = bcwin_ref.shape[2] // (2 * state)
    per = heads // groups
    span = per * size
    n_chunk = inner // CHUNK
    in_chunk = CHUNK // span
    block = mixed_ref.shape[1]

    kv, tp = lax.axis_index("kv"), lax.axis_index("tp")
    side, core = tp // 2, lax.rem(tp, 2)
    core_peer, x_peer = flip(tp, 1), flip(tp, 2)
    ranks = list(range(0, n_kv - 1, 2))
    ranks = ranks[: len(ranks) // 2] + ranks[: len(ranks) // 2 - 1 : -1] + list(range(1, n_kv - 1, 2))
    exits = [i + (i - kv + n_kv) // n_kv for i in ranks]

    hid_copy = pltpu.make_async_copy(hid_hbm, hid, hid_sem.at[0])
    hid_copy.start()
    gin_copy = pltpu.make_async_copy(gin_hbm, gin_ref, hid_sem.at[1])
    gin_copy.start()
    dtw_copy = pltpu.make_async_copy(dtw_hbm, dtw.at[pl.ds(0, heads)], hid_sem.at[2])
    dtw_copy.start()
    barrier = pltpu.get_barrier_semaphore()
    for device in [{"tp": core_peer}, {"tp": x_peer}] + [{"kv": p} for p in exits]:
        pl.semaphore_signal(barrier, inc=1, device_id=device, device_id_type=pl.DeviceIdType.MESH)

    w_copies = [
        pltpu.make_async_copy(src.at[:, pl.ds(j * CHUNK, CHUNK)], wbuf.at[i], w_sem.at[i])
        for i, (src, j) in enumerate(
            [(src, j) for src in (bcw_hbm, xw_hbm, zw_hbm) for j in range(n_chunk)])
    ]
    for copy in w_copies:
        copy.start()
    small_copies = [
        pltpu.make_async_copy(src, dst, small_sem.at[i])
        for i, (src, dst) in enumerate([
            (acc_hbm, acc_smem), (bias_hbm, bias_smem), (decay_hbm, decay_smem), (skip_hbm, skip_smem),
            (xh_hbm, xh_ref), (bch_hbm, bch_ref), (xk_hbm, xk_ref), (bck_hbm, bck_ref),
            (gain_hbm, gain_ref)])]
    for copy in small_copies:
        copy.start()
    n_big = len(w_copies)

    dtw[heads:] = jnp.zeros((dtw.shape[0] - heads, dtw.shape[1]), dtw.dtype)
    hid_copy.wait()
    lanes = entry32.shape[2]
    for i in range(entry32.shape[0]):
        entry32[i] = hid[:, i * lanes : (i + 1) * lanes].astype(jnp.float32)
    gin_copy.wait()
    gin = gin_ref[...].astype(jnp.float32).reshape(1, -1)
    entry, squares = [], []
    for p in range(tokens // rows):
        for t in range(props):
            v = jnp.concatenate(
                [entry32[i, pl.ds(p * rows + t, seqs, stride=props), :] for i in range(entry32.shape[0])],
                axis=1)
            squares.append(jnp.sum(v * v, axis=1, keepdims=True))
            entry.append(v * gin)
    entry = jnp.concatenate(entry, axis=0).astype(jnp.bfloat16)
    squares = jnp.concatenate(squares, axis=0)
    high = squares.astype(jnp.bfloat16).astype(jnp.float32)

    saved_copies = [
        pltpu.make_async_copy(saved_hbm.at[s], saved[s], saved_sem.at[s]) for s in range(seqs)]
    ow_copies = [
        pltpu.make_async_copy(
            w_hbm.at[:, pl.ds(pl.multiple_of(p * block, block), block)], w_buf.at[i], ow_sem.at[i])
        for i, p in enumerate(exits + [kv])]

    def put(ref, value):
        for p in range(tokens // rows):
            ref[(p % 2) * 2 + p // 2] = value[p * rows : (p + 1) * rows].astype(jnp.bfloat16)

    def core_copy(k):
        src, dst = (prod_dt, peer_dt) if k < 0 else (prod.at[k], peer.at[k])
        return remote(
            src.at[pl.ds(2 - 2 * core, 2)], dst, c_send.at[k + 1], c_recv.at[k + 1], {"tp": core_peer})

    def x_copy(k):
        src, dst = (half_dt, far_dt) if k < 0 else (half.at[k], far.at[k])
        return remote(src, dst, x_send.at[k + 1], x_recv.at[k + 1], {"tp": x_peer})

    def forward(k):
        core_copy(k).wait_recv()
        mine, theirs, send, keep = (prod_dt, peer_dt, half_dt, own_dt) if k < 0 else (
            prod.at[k], peer.at[k], half.at[k], own.at[k])
        away = mine[2 * core + 1 - side].astype(jnp.float32) + theirs[1 - side].astype(jnp.float32)
        send[...] = away.astype(jnp.bfloat16)
        x_copy(k).start()
        keep[...] = mine[2 * core + side].astype(jnp.float32) + theirs[side].astype(jnp.float32)

    dtw_copy.wait()
    lane = lax.broadcasted_iota(jnp.int32, (tokens, 128), 1)
    first = dot(entry, dtw[...], NT)
    first = jnp.where(lane == 126, high, jnp.where(lane == 127, squares - high, first))
    put(prod_dt, first)
    pl.semaphore_wait(barrier, 2 + len(exits))
    core_copy(-1).start()
    for k in range(n_big):
        w_copies[k].wait()
        put(prod.at[k], dot(entry, wbuf[k]))
        core_copy(k).start()
        if k >= LAG - 1:
            forward(k - LAG)
        if k == 0:
            for copy in saved_copies:
                copy.start()
    for k in range(n_big - LAG, n_big):
        forward(k)
    for copy in ow_copies:
        copy.start()

    for copy in small_copies:
        copy.wait()
    seq_at = lax.broadcasted_iota(jnp.int32, (seqs, CHUNK), 0)
    acc = jnp.zeros((seqs, CHUNK), jnp.int32)
    for s in range(seqs):
        acc = jnp.where(seq_at == s, acc_smem[s], acc)
    picks = [acc == j for j in range(props + 1)]
    eh = lax.broadcasted_iota(jnp.int32, (128, inner), 0)
    ec = lax.broadcasted_iota(jnp.int32, (128, inner), 1)
    expand = (eh == ec // size).astype(jnp.float32)
    lane_at = lax.broadcasted_iota(jnp.int32, (8, 128), 1)
    row_at = lax.broadcasted_iota(jnp.int32, (8, 128), 0)
    par = jnp.zeros((8, 128), jnp.float32)
    for i, smem in enumerate((bias_smem, decay_smem, skip_smem)):
        for h in range(heads):
            par = jnp.where((row_at == i) & (lane_at == h), smem[h], par)
    wide = dot(par, expand, precision=lax.Precision.HIGHEST)
    bias, rate, skip = wide[0:1], jnp.exp(wide[1:2]), wide[2:3]
    row = lax.broadcasted_iota(jnp.int32, (rows, state), 0)

    def total(k):
        x_copy(k).wait_recv()
        if k < 0:
            return own_dt[...] + far_dt[...].astype(jnp.float32)
        return own[k] + far[k].astype(jnp.float32)

    head_part = total(-1)
    sums = head_part[:, 126:127] + head_part[:, 127:128]
    scale = lax.rsqrt(sums / features + EPSILON)

    def fresh(k):
        v = (total(k) * scale).astype(jnp.bfloat16).astype(jnp.float32)
        return [v[t * seqs : (t + 1) * seqs] for t in range(props)]

    def conv(hist_ref, tap_ref, out_ref, rows_fresh, lo):
        kept = hist_ref.shape[0] - props
        hist = [hist_ref[m, :, lo : lo + CHUNK].astype(jnp.float32) for m in range(hist_ref.shape[0])]
        win = []
        for k in range(kept):
            v = hist[k]
            for j in range(1, props + 1):
                v = jnp.where(picks[j], hist[j + k], v)
            win.append(v)
        win += rows_fresh
        for m, v in enumerate(win):
            out_ref[m, :, lo : lo + CHUNK] = v.astype(jnp.bfloat16)
        taps = [tap_ref[j : j + 1, lo : lo + CHUNK].astype(jnp.float32) for j in range(tap_ref.shape[0])]
        out = []
        for t in range(props):
            v = win[t] * taps[0]
            for j in range(1, len(taps)):
                v = v + win[t + j] * taps[j]
            out.append(silu(v))
        return out

    dt_raw = (head_part * scale).astype(jnp.bfloat16)
    dtw_wide = dot(dt_raw, expand.astype(jnp.bfloat16))
    head_lane = lax.broadcasted_iota(jnp.int32, (rows, 128), 1)
    raw = jnp.where(head_lane < heads, dt_raw.astype(jnp.float32), 0.0)
    a_ref[...] = jnp.exp(-jnp.exp(par[1:2]) * softplus(raw + par[0:1]))

    b_terms, c_low, pairs = [], [], []
    for j in range(n_chunk):
        bc = conv(bch_ref, bck_ref, bcwin_ref, fresh(j), j * CHUNK)
        for i in range(CHUNK // (2 * state)):
            b = [v[:, 2 * i * state : (2 * i + 1) * state] for v in bc]
            c = [v[:, (2 * i + 1) * state : (2 * i + 2) * state] for v in bc]
            g = len(c_low)
            b_ref[:, g * state : (g + 1) * state] = jnp.concatenate(b, axis=0).astype(jnp.bfloat16)
            c_low.append(jnp.concatenate(c, axis=0).astype(jnp.bfloat16))
            pairs.append({
                (t, r): jnp.broadcast_to(jnp.sum(c[t] * b[r], axis=1, keepdims=True), (seqs, span))
                for t in range(props) for r in range(t + 1)})

    outs, gated_parts = [], []
    for j in range(n_chunk):
        lo = j * CHUNK
        sl = slice(lo, lo + CHUNK)
        xc = conv(xh_ref, xk_ref, xwin_ref, fresh(n_chunk + j), lo)
        sizes = [
            softplus(dtw_wide[t * seqs : (t + 1) * seqs, sl] + bias[:, sl]) for t in range(props)]
        xdt = [xc[t] * sizes[t] for t in range(props)]
        xdt_ref[:, sl] = jnp.concatenate(xdt, axis=0).astype(jnp.bfloat16)
        decays = [-rate[:, sl] * v for v in sizes]
        out_t = []
        for t in range(props):
            gap = decays[t]
            out = skip[:, sl] * xc[t]
            for r in range(t, -1, -1):
                pair = jnp.concatenate(
                    [pairs[j * in_chunk + i][(t, r)] for i in range(in_chunk)], axis=1)
                if r == t:
                    out = out + pair * xdt[r]
                else:
                    out = out + jnp.exp(gap) * pair * xdt[r]
                    gap = gap + decays[r]
            out_t.append((out, jnp.exp(gap)))
        outs.append(out_t)

    carried = [jnp.zeros((rows, span), jnp.float32) for _ in range(groups)]
    for s in range(seqs):
        saved_copies[s].wait()
        s0 = saved[s][acc_smem[s]]
        s0_ref[s] = s0
        low = s0.reshape(heads * size, state).astype(jnp.bfloat16)
        for g in range(groups):
            masked = jnp.where(row % seqs == s, c_low[g].astype(jnp.float32), 0.0).astype(jnp.bfloat16)
            carried[g] = carried[g] + dot(masked, low[g * span : (g + 1) * span], NT)

    square_sums = [jnp.zeros((seqs, 1), jnp.float32) for _ in range(props)]
    gain = gain_ref[...].astype(jnp.float32).reshape(1, inner)
    for j in range(n_chunk):
        sl = slice(j * CHUNK, (j + 1) * CHUNK)
        zs = fresh(2 * n_chunk + j)
        scaled_t = []
        for t in range(props):
            held = jnp.concatenate(
                [carried[j * in_chunk + i][t * seqs : (t + 1) * seqs] for i in range(in_chunk)], axis=1)
            out, fade = outs[j][t]
            v = (out + fade * held) * silu(zs[t])
            square_sums[t] = square_sums[t] + jnp.sum(v * v, axis=1, keepdims=True)
            scaled_t.append((v * gain[:, sl]).astype(jnp.bfloat16))
        gated_parts.append(jnp.concatenate(scaled_t, axis=0))
    scaled = jnp.concatenate(gated_parts, axis=1)

    diagonal = lax.broadcasted_iota(jnp.int32, (rows, 128), 0) == lax.broadcasted_iota(
        jnp.int32, (rows, 128), 1)
    norm_row = jnp.sum(
        jnp.where(diagonal, jnp.concatenate(square_sums, axis=0), 0.0), axis=0, keepdims=True)
    norm_out[...] = norm_row
    n_copies = [
        remote(norm_out, norm_in.at[kv], n_send.at[i], n_recv.at[kv], {"kv": p})
        for i, p in enumerate(exits)]
    for copy in n_copies:
        copy.start()
    o_copies = [
        remote(part.at[i], slots.at[kv], o_send.at[i], o_recv.at[kv], {"kv": p})
        for i, p in enumerate(exits)]
    sources = [flip(kv, d) for d in range(1, n_kv)]

    def arrived(p):
        remote(norm_out, norm_in.at[p], n_send.at[0], n_recv.at[p], {"kv": p}).wait_recv()

    def landed(p):
        remote(part.at[0], slots.at[p], o_send.at[0], o_recv.at[p], {"kv": p}).wait_recv()

    for i in range(n_kv):
        ow_copies[i].wait()
        value = dot(scaled, w_buf[i])
        if i < n_kv - 1:
            part[i] = value.astype(jnp.bfloat16)
            o_copies[i].start()
    for p in sources:
        arrived(p)
        norm_row = norm_row + norm_in[p]
    norm = lax.rsqrt(
        jnp.sum(jnp.where(diagonal, norm_row, 0.0), axis=1, keepdims=True) / channels + EPSILON)
    for p in sources:
        landed(p)
        value = value + slots[p].astype(jnp.float32)
    value = value * norm
    for i in range(fin.shape[0]):
        for t in range(props):
            fin[i, pl.ds(t, seqs, stride=props), :] = value[
                t * seqs : (t + 1) * seqs, i * lanes : (i + 1) * lanes]
        mixed_ref[:, i * lanes : (i + 1) * lanes] = fin[i].astype(mixed_ref.dtype)
    for k in range(-1, n_big):
        core_copy(k).wait_send()
        x_copy(k).wait_send()
    for copy in n_copies + o_copies:
        copy.wait_send()


def write_kernel(
    mixed_ref, s0_ref, xdt_ref, b_ref, a_ref, xwin_ref, bcwin_ref,
    mixed_out, states_out, xwin_out, bcwin_out,
    a_smem, new, a_sem, small_sem, first_sem, new_sem,
):
    seqs, heads, size, state = s0_ref.shape
    rows = b_ref.shape[0]
    props = rows // seqs
    groups = b_ref.shape[1] // state
    per = heads // groups
    span = per * size
    a_copy = pltpu.make_async_copy(a_ref, a_smem, a_sem)
    a_copy.start()
    copies = [
        pltpu.make_async_copy(s0_ref.at[s], states_out.at[s, 0], first_sem.at[s]) for s in range(seqs)]
    copies += [
        pltpu.make_async_copy(src, dst, small_sem.at[i])
        for i, (src, dst) in enumerate(
            [(mixed_ref, mixed_out), (xwin_ref, xwin_out), (bcwin_ref, bcwin_out)])]
    for copy in copies:
        copy.start()
    row = lax.broadcasted_iota(jnp.int32, (rows, state), 0)
    a_copy.wait()
    turned = [
        jnp.transpose(xdt_ref[:, g * span : (g + 1) * span].astype(jnp.float32)).astype(jnp.bfloat16)
        for g in range(groups)]

    def new_copy(s):
        return pltpu.make_async_copy(
            new.at[s], states_out.at[s, pl.ds(1, props)], new_sem.at[s])

    for s in range(seqs):
        for g in range(groups):
            b = b_ref[:, g * state : (g + 1) * state].astype(jnp.float32)
            masked = jnp.concatenate(
                [jnp.where(row == t * seqs + s, b, 0.0) for t in range(props)],
                axis=1).astype(jnp.bfloat16)
            outer = dot(turned[g], masked)
            for h in range(per):
                head = g * per + h
                now = s0_ref[s, head]
                for t in range(props):
                    now = a_smem[t * seqs + s, head] * now + outer[
                        h * size : (h + 1) * size, t * state : (t + 1) * state]
                    new[s, t, head] = now
        new_copy(s).start()
    for copy in copies:
        copy.wait()
    for s in range(seqs):
        new_copy(s).wait()


def local(
    hidden, input_gain, x_weight, z_weight, bc_weight, dt_weight, x_kernel, bc_kernel,
    dt_bias, decay_log, skip_scale, output_gain, output_weight, saved_states,
    x_history, bc_history, accepted,
):
    heads = dt_bias.shape[0]
    seqs, kept, _, size, state = saved_states.shape
    hist = x_history.shape[1]
    tokens, depth = hidden.shape
    inner, bcw = x_weight.shape[1], bc_weight.shape[1]
    n_kv, n_tp = lax.axis_size("kv"), lax.axis_size("tp")
    rows = tokens // n_tp
    props = rows // seqs
    block = output_weight.shape[1] // n_kv
    n_big = 3 * inner // CHUNK
    f32, bf16 = jnp.float32, jnp.bfloat16

    vmem = pl.BlockSpec(memory_space=pltpu.VMEM)
    anym = pl.BlockSpec(memory_space=pl.ANY)
    dma = pltpu.SemaphoreType.DMA
    shapes = (
        ((rows, block), bf16), ((seqs, heads, size, state), f32), ((rows, inner), bf16),
        ((rows, bcw // 2), bf16), ((rows, 128), f32), ((hist, seqs, inner), bf16),
        ((hist, seqs, bcw), bf16))
    middle = pl.pallas_call(
        functools.partial(main_kernel, depth * n_tp, inner * n_kv, n_kv),
        out_shape=tuple(pltpu.VMEM(*s) for s in shapes),
        in_specs=[pl.BlockSpec(memory_space=pltpu.HBM)] * 17,
        out_specs=[vmem] * len(shapes),
        scratch_shapes=[
            pltpu.SMEM((seqs,), jnp.int32),
            pltpu.SMEM((heads,), f32),
            pltpu.SMEM((heads,), f32),
            pltpu.SMEM((heads,), f32),
            pltpu.VMEM((depth,), bf16),
            pltpu.VMEM((hist, seqs, inner), bf16),
            pltpu.VMEM((hist, seqs, bcw), bf16),
            pltpu.VMEM(x_kernel.shape, bf16),
            pltpu.VMEM(bc_kernel.shape, bf16),
            pltpu.VMEM((inner,), bf16),
            pltpu.VMEM((tokens, depth), bf16),
            pltpu.VMEM((depth // 128, tokens, 128), f32),
            pltpu.VMEM((128, depth), bf16),
            pltpu.VMEM((n_big, depth, CHUNK), bf16),
            pltpu.VMEM((n_tp, rows, 128), bf16),
            pltpu.VMEM((n_big, n_tp, rows, CHUNK), bf16),
            pltpu.VMEM((2, rows, 128), bf16),
            pltpu.VMEM((n_big, 2, rows, CHUNK), bf16),
            pltpu.VMEM((rows, 128), bf16),
            pltpu.VMEM((n_big, rows, CHUNK), bf16),
            pltpu.VMEM((rows, 128), f32),
            pltpu.VMEM((n_big, rows, CHUNK), f32),
            pltpu.VMEM((rows, 128), bf16),
            pltpu.VMEM((n_big, rows, CHUNK), bf16),
            pltpu.VMEM((n_kv, inner, block), bf16),
            pltpu.VMEM((n_kv - 1, rows, block), bf16),
            pltpu.VMEM((n_kv, rows, block), bf16),
            pltpu.VMEM((1, 128), f32),
            pltpu.VMEM((n_kv, 1, 128), f32),
            pltpu.VMEM((block // 128, rows, 128), f32),
            dma((3,)), dma((9,)), dma((n_big,)), dma((seqs,)), dma((n_kv,)),
            dma((n_big + 1,)), dma((n_big + 1,)), dma((n_big + 1,)), dma((n_big + 1,)),
            dma((n_kv - 1,)), dma((n_kv,)), dma((n_kv - 1,)), dma((n_kv,)),
        ] + [pltpu.VMEM((kept, heads, size, state), f32)] * seqs,
        compiler_params=pltpu.CompilerParams(
            vmem_limit_bytes=48 << 20, collective_id=0, has_side_effects=True),
        cost_estimate=pl.CostEstimate(
            flops=2 * tokens * depth * 3 * inner, bytes_accessed=36 << 20, transcendentals=0),
        name="mixer",
    )(*[pltpu.with_memory_space_constraint(v, pltpu.HBM) for v in (
        accepted, dt_bias, decay_log, skip_scale,
        hidden, input_gain, x_weight, z_weight, bc_weight, dt_weight.T,
        x_history.transpose(1, 0, 2), bc_history.transpose(1, 0, 2),
        x_kernel, bc_kernel, output_gain, saved_states, output_weight,
    )])
    mixed, new_states, xw, bcw_out = pl.pallas_call(
        write_kernel,
        out_shape=(
            jax.ShapeDtypeStruct((rows, block), bf16),
            jax.ShapeDtypeStruct(saved_states.shape, f32),
            jax.ShapeDtypeStruct((hist, seqs, inner), bf16),
            jax.ShapeDtypeStruct((hist, seqs, bcw), bf16)),
        in_specs=[vmem] * len(shapes),
        out_specs=[anym] * 4,
        scratch_shapes=[
            pltpu.SMEM((rows, 128), f32),
            pltpu.VMEM((seqs, props, heads, size, state), f32),
            dma, dma((3,)), dma((seqs,)), dma((seqs,)),
        ],
        compiler_params=pltpu.CompilerParams(vmem_limit_bytes=32 << 20),
        cost_estimate=pl.CostEstimate(
            flops=2 * saved_states.size, bytes_accessed=6 * saved_states.size, transcendentals=0),
        name="write",
    )(*[pltpu.with_memory_space_constraint(v, pltpu.VMEM) for v in middle])
    return (mixed, new_states, xw.transpose(1, 0, 2), bcw_out.transpose(1, 0, 2))


def fits(mesh):
    n_kv, n_tp = mesh.shape["kv"], mesh.shape["tp"]
    inner = INNER // n_kv
    return inner % 1024 == 0 and n_kv > 1 and n_kv & (n_kv - 1) == 0 and n_tp == 4


def solution(mesh):
    in_specs = (
        P(None, "tp"),
        P("tp"),
        P("tp", "kv"),
        P("tp", "kv"),
        P("tp", "kv"),
        P("tp", "kv"),
        P(None, "kv"),
        P(None, "kv"),
        P("kv"),
        P("kv"),
        P("kv"),
        P("kv"),
        P("kv", None),
        P("tp", None, "kv", None, None),
        P("tp", None, "kv"),
        P("tp", None, "kv"),
        P("tp"),
    )
    out_specs = (
        P("tp", "kv"),
        P("tp", None, "kv", None, None),
        P("tp", None, "kv"),
        P("tp", None, "kv"),
    )
    body = local if fits(mesh) else local_general
    return jax.shard_map(body, mesh=mesh, in_specs=in_specs, out_specs=out_specs, check_vma=False)
```
